32 devices in a mesh: sp: 8 (over z, x), tp: 4 (over y, core).
Axes of the slice: x: 2, y: 2, z: 4, core: 2. Of those that a mesh axis runs over, the one named last changes fastest.
Arguments:
- queries: bfloat16 [1024, 2048], P('sp', 'tp'), may hold values from -440 to 440
- key_rows: bfloat16 [1024, 1024], P('sp', 'tp'), may hold values from -6 to 6
- value_rows: bfloat16 [1024, 1024], P('sp', 'tp'), may hold values from -6 to 6
- sink_logits: float32 [32], P('tp'), may hold values from -6 to 6
- out_weight: bfloat16 [2048, 2048], P('tp'), may hold values from -0.125 to 0.125
- residual: bfloat16 [1024, 2048], P('sp'), may hold values from -3 to 3
- norm_gain: float32 [2048], replicated, may hold values from 0.1 to 1.9
- routes: int32 [1024, 2], P('sp'), may hold values from 0 to 7, all different within a row; in each aligned block of 128 rows (0 to 127, 128 to 255, ...) at most 64 rows name the same one
- route_weights: float32 [1024, 2], P('sp'), may hold values from 0.2 to 1
- gate_weight: bfloat16 [8, 2048, 4096], P('sp', None, 'tp'), may hold values from -0.125 to 0.125
- up_weight: bfloat16 [8, 2048, 4096], P('sp', None, 'tp'), may hold values from -0.125 to 0.125
- down_weight: bfloat16 [8, 4096, 2048], P('sp', 'tp'), may hold values from -0.09375 to 0.09375
Outputs:
- layer_out: bfloat16 [1024, 2048], P('sp')
The draws below stay inside these ranges and needn't reach their ends.
Inputs may be any that keep to these rules, and one draw needn't show every extreme that they name: `routes`: each row names 2 different experts. In each aligned block of 128 rows (the rows of one index of sp) no expert is named by more than 64 rows, a bound that some block reaches.
All inputs are finite; a program needn't handle non-finite values.
Results may differ from the reference program's by a relative error of at most 0.02.
Values may be sent and summed in bfloat16 or wider, within the bound.
A program may use at most 64 MiB of HBM per device.

```python
import math
import jax
import jax.numpy as jnp
import numpy as np
from jax import lax

D = 2048
HEAD_DIM = 64
QH = 32
KVH = 16
WINDOW = 128
FF = 4096
TOP = 2
TOK_DEV = 128
TOKENS = 1024
EXPERTS = 8
CAP = 64
N_SP = 8
N_TP = 4


def plant_keys(key):
    key_draw = jax.random.normal(jax.random.fold_in(key, 7), (TOKENS, KVH * HEAD_DIM), jnp.float32)
    return jnp.clip(key_draw, -6.0, 6.0)


def draw_key_rows(key, part):
    key_draw = plant_keys(key)
    return key_draw.astype(jnp.bfloat16)


def draw_queries(key, part):
    base = jax.random.normal(jax.random.fold_in(key, 8), (TOKENS, QH * HEAD_DIM), jnp.float32)
    base = jnp.clip(base, -6.0, 6.0)
    return base.astype(jnp.bfloat16)


def levels(key, extent, cuts, smallest, top_value):
    level = 1.0
    for axis_at, shards_of in cuts:
        steps = jax.random.uniform(jax.random.fold_in(jax.random.fold_in(key, 6), axis_at), (shards_of,), jnp.float32, smallest / len(cuts), top_value / len(cuts))
        level = level * jnp.repeat(jnp.exp(steps), extent[axis_at] // shards_of).reshape((-1,) + (1,) * (len(extent) - 1 - axis_at))
    return level


def deal_out(rng, own, number, rows, amount, top, limit, skew):
    ranking = jax.random.permutation(rng, amount)
    heavy_load, common = portions_of(amount, rows * top, limit, skew, True), portions_of(amount, rows * top, limit, skew, False)
    places = jnp.arange(amount)

    def named(tallies, turn):
        used = int((tallies > 0).sum())
        fixed = max(1, used // 4)
        moved = fixed + (places - fixed + turn * (used - fixed)) % max(1, amount - fixed)
        return jnp.zeros((amount,), jnp.int32).at[ranking[jnp.where(places < fixed, places, moved)]].set(jnp.asarray(tallies, jnp.int32))

    tallies = jnp.where(number % 4 == 0, named(heavy_load, number // 4), named(common, number - number // 4 - 1))
    mixed = jax.random.permutation(jax.random.fold_in(own, 3), amount)
    source_of, taker = mixed[0:amount // 2 * 2:2], mixed[1:amount // 2 * 2:2]
    margin = jnp.minimum(tallies[source_of] - 1, limit - tallies[taker]) // 2
    margin = jnp.where((source_of == ranking[0]) | (taker == ranking[0]) | (tallies[taker] == 0), 0, jnp.maximum(margin, 0))
    moved = jax.random.randint(jax.random.fold_in(own, 4), (amount // 2,), 0, 1 << 20) % (margin + 1)
    tallies = tallies.at[source_of].add(-moved).at[taker].add(moved)
    items = jnp.searchsorted(jnp.cumsum(tallies), jnp.arange(rows * top), side="right").astype(jnp.int32)
    grid = items.reshape(top, rows).T
    grid = grid[jax.random.permutation(jax.random.fold_in(own, 1), rows)]
    turn = jax.random.randint(jax.random.fold_in(own, 2), (rows, 1), 0, top)
    return jnp.take_along_axis(grid, (jnp.arange(top)[None, :] + turn) % top, axis=1)


def portions_of(amount, total, limit, slope, full):
    weights = [(1 << 20) // math.isqrt(standing ** slope) + 1 for standing in range(1, amount + 1)]
    largest = limit if full else min(limit, max(-(-total // amount), total * weights[0] // sum(weights)))
    least = 1 if total - largest >= amount - 1 else 0
    counts, surplus = [largest] + [least] * (amount - 1), total - largest - least * (amount - 1)
    while surplus > 0:
        movable = [i for i in range(1, amount) if counts[i] < largest] or [i for i in range(1, amount) if counts[i] < limit]
        whole, left = sum([weights[i] for i in movable]), surplus
        for i in movable:
            addition = min(limit - counts[i], max(1, left * weights[i] // whole), surplus)
            counts[i] = counts[i] + addition
            surplus = surplus - addition
    return np.array(counts)


def noise(rng, extent, deviation, limit, shards=(), kind=jnp.bfloat16):
    level = levels(rng, extent, shards, -0.22, 0.18) if shards else 1.0
    result = jax.random.normal(rng, extent, jnp.float32) * deviation * level
    return jnp.minimum(jnp.maximum(result, -limit), limit).astype(kind)


def setup_inputs(seed: int = 0) -> dict:
    key_of = jax.random.split(jax.random.key(seed), 13)
    queries = draw_queries(jax.random.fold_in(key_of[12], 71), 0)
    key_rows = draw_key_rows(jax.random.fold_in(key_of[12], 71), 0)
    value_rows = noise(key_of[2], (TOKENS, KVH * HEAD_DIM), 1.0, 6.0, ((0, 8), (1, 4)))
    sink_logits = noise(key_of[3], (QH,), 2.0, 6.0, ((0, 4),), jnp.float32)
    out_weight = noise(key_of[4], (QH * HEAD_DIM, D), (QH * HEAD_DIM) ** -0.5, 0.125, ((0, 4),))
    residual = noise(key_of[5], (TOKENS, D), 0.5, 3.0, ((0, 8),))
    norm_gain = jnp.clip(1.0 + 0.18 * jax.random.normal(key_of[6], (D,), jnp.float32), 0.1, 1.9)
    routes_keys = jax.random.split(jax.random.fold_in(key_of[7], 1), TOKENS // TOK_DEV)
    routes_turns = jax.random.permutation(jax.random.fold_in(key_of[7], 3), TOKENS // TOK_DEV)
    routes = jax.vmap(lambda own, number: deal_out(jax.random.fold_in(key_of[7], 2), own, number, TOK_DEV, EXPERTS, TOP, CAP, 1))(routes_keys, routes_turns).reshape((TOKENS, TOP))
    route_weights = jnp.clip(0.2 + 0.8 * jax.random.uniform(key_of[8], (TOKENS, TOP), jnp.float32) ** levels(key_of[8], (TOKENS, TOP), ((0, 8),), -0.2, 0.2), 0.2, 1.0)
    gate_weight = noise(key_of[9], (EXPERTS, D, FF), D ** -0.5, 0.125, ((0, 8), (2, 4)))
    up_weight = noise(key_of[10], (EXPERTS, D, FF), D ** -0.5, 0.125, ((0, 8), (2, 4)))
    down_weight = noise(key_of[11], (EXPERTS, FF, D), FF ** -0.5, 0.09375, ((0, 8), (1, 4)))
    return dict(queries=queries, key_rows=key_rows, value_rows=value_rows, sink_logits=sink_logits, out_weight=out_weight, residual=residual, norm_gain=norm_gain, routes=routes, route_weights=route_weights, gate_weight=gate_weight, up_weight=up_weight, down_weight=down_weight)


def reference(queries, key_rows, value_rows, sink_logits, out_weight, residual, norm_gain, routes, route_weights, gate_weight, up_weight, down_weight):
    blocks = TOKENS // WINDOW
    group_size = QH // KVH
    zeros_rim = jnp.zeros((WINDOW, KVH * HEAD_DIM), jnp.bfloat16)
    key_ext = jnp.concatenate([zeros_rim, key_rows], axis=0).reshape(blocks + 1, WINDOW, KVH, HEAD_DIM)
    val_ext = jnp.concatenate([zeros_rim, value_rows], axis=0).reshape(blocks + 1, WINDOW, KVH, HEAD_DIM)
    key_pair = jnp.concatenate([key_ext[:-1], key_ext[1:]], axis=1)
    val_pair = jnp.concatenate([val_ext[:-1], val_ext[1:]], axis=1)
    query_blocks = queries.reshape(blocks, WINDOW, KVH, group_size, HEAD_DIM)
    distance = jnp.arange(WINDOW)[:, None] + WINDOW - jnp.arange(2 * WINDOW)[None, :]
    key_global = jnp.arange(blocks)[:, None, None] * WINDOW + jnp.arange(2 * WINDOW)[None, None, :] - WINDOW
    allowed = (distance >= 0)[None] & (distance <= WINDOW)[None] & (key_global >= 0)
    head_ids = jnp.arange(QH)
    slopes = jnp.exp2(-8.0 * (head_ids + 1).astype(jnp.float32) / QH).reshape(KVH, group_size)

    def attend_head(inputs):
        q_head, k_head, v_head, sink_head, slope_head = inputs
        scores = jnp.einsum('bqgd,bcd->bgqc', q_head.astype(jnp.float32), k_head.astype(jnp.float32)) * HEAD_DIM ** (-0.5)
        scores = scores - slope_head[None, :, None, None] * distance.astype(jnp.float32)
        scores = jnp.where(allowed[:, None], scores, -jnp.inf)
        row_peak = lax.optimization_barrier(jnp.max(scores, axis=-1, keepdims=True))
        log_total = row_peak + jnp.log(lax.optimization_barrier(jnp.sum(jnp.exp(scores - row_peak), axis=-1, keepdims=True)))
        probs = jnp.exp(scores - log_total).astype(jnp.bfloat16)
        mixed = jnp.einsum('bgqc,bcd->bqgd', probs.astype(jnp.float32), v_head.astype(jnp.float32))
        keep_factor = jax.nn.sigmoid(log_total[..., 0] - sink_head[None, :, None])
        keep_factor = jnp.transpose(keep_factor, (0, 2, 1))[..., None]
        return (mixed * keep_factor).astype(jnp.bfloat16)
    per_head = lax.map(attend_head, (jnp.moveaxis(query_blocks, 2, 0), jnp.moveaxis(key_pair, 2, 0), jnp.moveaxis(val_pair, 2, 0), sink_logits.reshape(KVH, group_size), slopes))
    attended = jnp.moveaxis(per_head, 0, 2).reshape(TOKENS, QH * HEAD_DIM)
    columns = QH * HEAD_DIM // N_TP
    head_total = jnp.zeros((TOKENS, D), jnp.float32)
    for piece_id in range(N_TP):
        partial_value = jnp.dot(attended[:, piece_id * columns:(piece_id + 1) * columns], out_weight[piece_id * columns:(piece_id + 1) * columns], preferred_element_type=jnp.float32)
        head_total = head_total + lax.optimization_barrier(partial_value.astype(jnp.bfloat16)).astype(jnp.float32)
    mixed_state = (residual.astype(jnp.float32) + head_total).astype(jnp.bfloat16)
    state32 = mixed_state.astype(jnp.float32)
    normed = (state32 * lax.rsqrt(lax.optimization_barrier(jnp.mean(state32 * state32, axis=-1, keepdims=True)) + 1e-06) * norm_gain).astype(jnp.bfloat16)
    slots = N_SP * CAP
    flat_routes = routes.reshape(-1).astype(jnp.int32)
    token_of = (jnp.arange(TOKENS * TOP) // TOP).astype(jnp.int32)
    member = (flat_routes[:, None] == jnp.arange(EXPERTS)[None, :]).astype(jnp.int32)
    slot_rank = lax.optimization_barrier(jnp.sum((jnp.cumsum(member, axis=0) - 1) * member, axis=1)).astype(jnp.int32)

    def one_expert(inputs):
        expert_id, w_gate, w_up, w_down = inputs
        target = jnp.where(flat_routes == expert_id, slot_rank, slots).astype(jnp.int32)
        slot_token = jnp.zeros((slots,), jnp.int32).at[target].set(token_of, mode='drop')
        slot_rows = normed[slot_token]
        gate_pre = jnp.dot(slot_rows, w_gate, preferred_element_type=jnp.float32)
        up_pre = jnp.dot(slot_rows, w_up, preferred_element_type=jnp.float32)
        activated = (jax.nn.silu(gate_pre) * up_pre).astype(jnp.bfloat16)
        act_groups = activated.reshape(slots, N_TP, FF // N_TP).astype(jnp.float32)
        down_groups = w_down.reshape(N_TP, FF // N_TP, D).astype(jnp.float32)
        parts = jnp.einsum('mpf,pfd->pmd', act_groups, down_groups)
        parts = lax.optimization_barrier(parts.astype(jnp.bfloat16)).astype(jnp.float32)
        return lax.optimization_barrier(jnp.sum(parts, axis=0)).astype(jnp.bfloat16)
    outputs = lax.map(one_expert, (jnp.arange(EXPERTS, dtype=jnp.int32), gate_weight, up_weight, down_weight))
    flat_index = (flat_routes * slots + slot_rank).astype(jnp.int32)
    picked = outputs.reshape(EXPERTS * slots, D)[flat_index].reshape(TOKENS, TOP, D)
    expert_mix = lax.optimization_barrier(jnp.sum(route_weights[..., None] * picked.astype(jnp.float32), axis=1))
    return (state32 + expert_mix).astype(jnp.bfloat16)
```

```python
import functools

import jax
import jax.numpy as jnp
import numpy as np
from jax import lax
from jax.experimental import pallas as pl
from jax.experimental.pallas import tpu as pltpu
from jax.sharding import PartitionSpec as P

HEAD_DIM = 64
WINDOW = 128
TOP = 2
CORES = 2
F32 = jnp.float32
BF16 = jnp.bfloat16
MESH = pl.DeviceIdType.MESH


def kernel(
    S,
    T,
    sink_hbm,
    q_hbm,
    k_hbm,
    v_hbm,
    res_hbm,
    gain_hbm,
    routes_hbm,
    rw_hbm,
    wo_hbm,
    wg_hbm,
    wu_hbm,
    wd_hbm,
    out_hbm,
    sink,
    q,
    k,
    v,
    res,
    gain,
    routes,
    rw,
    wo,
    wg,
    wu,
    wd,
    halo,
    att,
    pp,
    rc1,
    sb1,
    ry1,
    mixed,
    picked,
    x_all,
    xn,
    act,
    yp,
    rc2,
    sb2,
    ry2,
    rb,
    ret,
    o_all,
    w_sem,
    halo_s,
    halo_r,
    c1_s,
    c1_r,
    y1_s,
    y1_r,
    a_s,
    a_r,
    fy_s,
    fy_r,
    fc_s,
    fc_r,
    c2_s,
    c2_r,
    y2_s,
    y2_r,
    b_s,
    b_r,
    gy_s,
    gy_r,
    gc_s,
    gc_r,
    o_sem,
):
    R, W = res.shape
    D = W * T
    Y = T // CORES
    H = q.shape[1] // HEAD_DIM
    KV = k.shape[1] // HEAD_DIM
    G = H // KV
    C = x_all.shape[0] // S
    Z = S // 2
    NEAR = (Z + 1) * C
    FL = wg.shape[1]
    NH = y1_s.shape[1]
    HW = W // NH

    me = lax.axis_index("sp")
    t = lax.axis_index("tp")
    y = t // CORES
    c = t % CORES
    oc = 1 - c
    z = me // 2
    x = me % 2

    def tp_of(yy, cc):
        return yy * CORES + cc

    def cols(tt):
        return pl.ds(pl.multiple_of(tt * W, W), W)

    def part(tt, j):
        return pl.ds(pl.multiple_of(tt * W + j * HW, HW), HW)

    def rows(s):
        return pl.ds(pl.multiple_of(s * C, C), C)

    def yo(d):
        return (y + d) % Y

    def remote(src, dst, ss, rs, **dev):
        return pltpu.make_async_remote_copy(
            src_ref=src, dst_ref=dst, send_sem=ss, recv_sem=rs, device_id=dev, device_id_type=MESH
        )

    def peer(p):
        zz = z
        bit = 1
        while bit < Z:
            if (p % Z) // bit % 2:
                zz = zz + bit * (1 - 2 * (zz // bit % 2))
            bit *= 2
        return 2 * zz + (x + p // Z) % 2

    far = list(range(Z + 1, 2 * Z))
    near = list(range(Z + 1))
    groups = ((0, near), (NEAR, far))

    def span(p):
        return pl.ds(p * C, C)

    def local(p):
        return pl.ds((p if p <= Z else p - Z - 1) * C, C)

    def group(p):
        return 0 if p <= Z else 1

    barrier = pltpu.get_barrier_semaphore()

    @pl.loop(1, S)
    def _(d):
        pl.semaphore_signal(
            barrier, inc=1, device_id={"sp": (me + d) % S}, device_id_type=MESH
        )

    for d in range(1, Y):
        pl.semaphore_signal(
            barrier, inc=1, device_id={"tp": tp_of(yo(d), c)}, device_id_type=MESH
        )
    pl.semaphore_signal(barrier, inc=1, device_id={"tp": tp_of(y, oc)}, device_id_type=MESH)

    loads = [
        pltpu.make_async_copy(src, dst, w_sem.at[i])
        for i, (src, dst) in enumerate(
            (
                (k_hbm, k),
                (v_hbm, v),
                (q_hbm, q),
                (routes_hbm, routes),
                (sink_hbm, sink),
                (res_hbm.at[:, cols(t)], res),
                (rw_hbm, rw),
                (gain_hbm, gain),
                (wo_hbm, wo),
                (wg_hbm.at[0], wg),
                (wu_hbm.at[0], wu),
                (wd_hbm.at[0], wd),
            )
        )
    ]
    for load in loads:
        load.start()
    loads[0].wait()
    loads[1].wait()
    pl.semaphore_wait(barrier, S - 1 + Y)

    halo_copies = [
        remote(src, halo.at[i], halo_s.at[i], halo_r.at[i], sp=jnp.minimum(me + 1, S - 1))
        for i, src in enumerate((k, v))
    ]

    @pl.when(me < S - 1)
    def _():
        for copy in halo_copies:
            copy.start()

    for load in loads[2:5]:
        load.wait()

    qi = lax.broadcasted_iota(jnp.int32, (R, R), 0)
    kj = lax.broadcasted_iota(jnp.int32, (R, R), 1)
    dist_own = (qi - kj).astype(F32)
    dist_old = (qi - kj + WINDOW).astype(F32)
    nt = (((1,), (1,)), ((), ()))

    ok_own = qi >= kj
    ok_old = (kj >= qi) & (kj + me * R >= WINDOW)

    base = jnp.float32(1.0)
    for i in range(1, T):
        base = jnp.where(t == i, jnp.float32(2.0 ** (-8.0 * i / T)), base)

    def head(h):
        return slice(h * HEAD_DIM, (h + 1) * HEAD_DIM), slice(
            (h // G) * HEAD_DIM, (h // G + 1) * HEAD_DIM
        )

    def scores(h, keys, dist, ok):
        raw = lax.dot_general(q[:, head(h)[0]], keys, nt, preferred_element_type=F32)
        slope = base * np.float32(2.0 ** (-8.0 * (h + 1) / (H * T)))
        return jnp.where(ok, raw * HEAD_DIM**-0.5 - slope * dist, -jnp.inf)

    own = []
    for h in range(H):
        s_own = scores(h, k[:, head(h)[1]], dist_own, ok_own)
        top = jnp.max(s_own, axis=1, keepdims=True)
        e_own = jnp.exp(s_own - top)
        own.append(
            (
                top,
                jnp.sum(e_own, axis=1, keepdims=True),
                jnp.dot(e_own.astype(BF16), v[:, head(h)[1]], preferred_element_type=F32),
            )
        )

    def column(row):
        return jnp.broadcast_to(row, (R, R)).T[:, 0:1]

    r0 = column(routes[0:1, :].astype(F32)).astype(jnp.int32)
    r1 = column(routes[1:2, :].astype(F32)).astype(jnp.int32)
    lane_e = lax.broadcasted_iota(jnp.int32, (R, 128), 1)
    hit0 = lane_e == r0
    hit1 = lane_e == r1
    member = jnp.where(hit0 | hit1, 1.0, 0.0).astype(BF16)
    tri = jnp.where(
        lax.broadcasted_iota(jnp.int32, (R, R), 1) < lax.broadcasted_iota(jnp.int32, (R, R), 0),
        1.0,
        0.0,
    ).astype(BF16)
    rank = jnp.dot(tri, member, preferred_element_type=F32)
    rank0 = jnp.sum(jnp.where(hit0, rank, 0.0), axis=1, keepdims=True)
    rank1 = jnp.sum(jnp.where(hit1, rank, 0.0), axis=1, keepdims=True)
    slot0 = r0.astype(F32) * C + rank0
    slot1 = r1.astype(F32) * C + rank1
    lane_s = lax.broadcasted_iota(jnp.int32, (R, S * C), 1).astype(F32)

    def picker(slot):
        return jnp.where(lane_s == slot, 1.0, 0.0)

    both = (picker(slot0) + picker(slot1)).T.astype(BF16)

    @pl.when(me > 0)
    def _():
        for copy in halo_copies:
            copy.wait_recv()

    @pl.when(me == 0)
    def _():
        halo[...] = jnp.zeros_like(halo)

    for h in range(H):
        hc, kc = head(h)
        top, weight, mix = own[h]
        s_old = scores(h, halo[0, :, kc], dist_old, ok_old)
        peak = jnp.maximum(top, jnp.max(s_old, axis=1, keepdims=True))
        shrink = jnp.exp(top - peak)
        e_old = jnp.exp(s_old - peak)
        total = weight * shrink + jnp.sum(e_old, axis=1, keepdims=True)
        mix = mix * shrink + jnp.dot(
            e_old.astype(BF16), halo[1, :, kc], preferred_element_type=F32
        )
        keep = 1.0 / (total + jnp.exp(sink[0:1, h : h + 1] - peak))
        att[:, hc] = (mix * keep).astype(BF16)

    for load in loads[5:9]:
        load.wait()

    def project(tt):
        pp[:, cols(tt)] = jnp.dot(att[...], wo[:, cols(tt)], preferred_element_type=F32).astype(
            BF16
        )

    def c1(yy):
        return remote(
            pp.at[:, cols(tp_of(yy, oc))], rc1.at[yy], c1_s.at[yy], c1_r.at[yy], tp=tp_of(y, oc)
        )

    def y1_send(yy, j):
        return remote(
            sb1.at[yy, j], ry1.at[y, j], y1_s.at[yy, j], y1_r.at[y, j], tp=tp_of(yy, c)
        )

    def y1_recv(yy, j):
        return remote(
            sb1.at[yy, j], ry1.at[yy, j], y1_s.at[yy, j], y1_r.at[yy, j], tp=tp_of(yy, c)
        )

    turns = list(range(1, Y)) + [0]

    def half(j):
        return slice(j * HW, (j + 1) * HW)

    for d in turns:
        project(tp_of(yo(d), oc))
        c1(yo(d)).start()
    for d in turns:
        project(tp_of(yo(d), c))
    for d in range(1, Y):
        c1(yo(d)).wait_recv()
        for j in range(NH):
            sb1[yo(d), j] = (
                pp[:, part(tp_of(yo(d), c), j)].astype(F32) + rc1[yo(d), :, half(j)].astype(F32)
            ).astype(BF16)
            y1_send(yo(d), j).start()
    c1(y).wait_recv()

    def a_send(p, j):
        e = peer(p)
        return remote(
            picked.at[rows(e), half(j)],
            x_all.at[span(p), part(t, j)],
            a_s.at[p, j],
            a_r.at[p, j],
            sp=e,
        )

    def fy_send(p, yy):
        ref = x_all.at[span(p), cols(t)]
        return remote(ref, ref, fy_s.at[p, yy], fy_r.at[p, y], tp=tp_of(yy, c))

    def fy_recv(p, yy):
        ref = x_all.at[span(p), cols(tp_of(yy, c))]
        return remote(ref, ref, fy_s.at[p, yy], fy_r.at[p, yy], tp=tp_of(yy, c))

    def fc_send(p, yy):
        ref = x_all.at[span(p), cols(tp_of(yy, c))]
        return remote(ref, ref, fc_s.at[p, yy], fc_r.at[p, yy], tp=tp_of(y, oc))

    def fc_recv(p, yy):
        ref = x_all.at[span(p), cols(tp_of(yy, oc))]
        return remote(ref, ref, fc_s.at[p, yy], fc_r.at[p, yy], tp=tp_of(y, oc))

    outward = [Z] + list(range(1, Z)) + far

    for j in range(NH):
        head_sum = pp[:, part(t, j)].astype(F32) + rc1[y, :, half(j)].astype(F32)
        for d in range(1, Y):
            y1_recv(yo(d), j).wait_recv()
            head_sum = head_sum + ry1[yo(d), j].astype(F32)
        mixed[:, half(j)] = (res[:, half(j)].astype(F32) + head_sum).astype(BF16)
        picked[:, half(j)] = jnp.dot(
            both, mixed[:, half(j)], preferred_element_type=F32
        ).astype(BF16)
        for p in outward:
            a_send(p, j).start()
    x_all[span(0), cols(t)] = picked[rows(me)]

    def forward(p):
        for d in range(1, Y):
            fy_send(p, yo(d)).start()
        fc_send(p, y).start()

    def relay(p):
        for i in range(1, Y):
            fy_recv(p, yo(i)).wait_recv()
            fc_send(p, yo(i)).start()

    def arrive(p):
        for j in range(NH):
            a_send(p, j).wait_recv()
        forward(p)

    def norm(p):
        for i in range(Y):
            fc_recv(p, yo(i)).wait_recv()
        wide = x_all[span(p)].astype(F32)
        scale = lax.rsqrt(jnp.mean(wide * wide, axis=1, keepdims=True) + 1e-06)
        xn[span(p)] = (wide * scale * gain[...]).astype(BF16)

    TN = min(256, FL)
    NT = FL // TN

    def hidden(g, hooks):
        first, places = groups[g]
        m = len(places) * C

        @pl.loop(0, NT)
        def _(n):
            nn = pl.ds(pl.multiple_of(n * TN, TN), TN)
            gate = jnp.dot(xn[first : first + m], wg[:, nn], preferred_element_type=F32)
            up = jnp.dot(xn[first : first + m], wu[:, nn], preferred_element_type=F32)
            act[0:m, nn] = (gate / (1.0 + jnp.exp(-gate)) * up).astype(BF16)
            for i in range(NT):
                todo = hooks[i * len(hooks) // NT : (i + 1) * len(hooks) // NT]
                if todo:

                    @pl.when(n == i)
                    def _(todo=todo):
                        for hook in todo:
                            hook()

    def c2(g, yy):
        m = len(groups[g][1]) * C
        return remote(
            yp.at[g, pl.ds(0, m), cols(tp_of(yy, oc))],
            rc2.at[g, yy, pl.ds(0, m)],
            c2_s.at[g, yy],
            c2_r.at[g, yy],
            tp=tp_of(y, oc),
        )

    def down_block(g, tt):
        m = len(groups[g][1]) * C
        yp[g, 0:m, cols(tt)] = jnp.dot(
            act[0:m], wd[:, cols(tt)], preferred_element_type=F32
        ).astype(BF16)

    def y2_send(p, yy):
        g = group(p)
        return remote(
            sb2.at[g, yy, local(p)],
            ry2.at[g, y, local(p)],
            y2_s.at[p, yy],
            y2_r.at[p, y],
            tp=tp_of(yy, c),
        )

    def y2_recv(p, yy):
        g = group(p)
        return remote(
            sb2.at[g, yy, local(p)],
            ry2.at[g, yy, local(p)],
            y2_s.at[p, yy],
            y2_r.at[p, yy],
            tp=tp_of(yy, c),
        )

    back = (list(range(2, Z)) + [1, Z, 0], far[1:] + far[:1])

    def pair_sum(g, d):
        yy = yo(d)
        c2(g, yy).wait_recv()
        for p in back[g]:
            sb2[g, yy, local(p)] = (
                yp[g, local(p), cols(tp_of(yy, c))].astype(F32)
                + rc2[g, yy, local(p)].astype(F32)
            ).astype(BF16)
            y2_send(p, yy).start()

    def down(g):
        held = None
        for d in turns:
            down_block(g, tp_of(yo(d), oc))
            c2(g, yo(d)).start()
            if held is not None:
                pair_sum(g, held)
            down_block(g, tp_of(yo(d), c))
            held = d
        c2(g, y).wait_recv()

    def b_send(p):
        e = peer(p)
        return remote(rb.at[span(p)], ret.at[rows(me)], b_s.at[p], b_r.at[p], sp=e)

    def b_recv(p):
        e = peer(p)
        return remote(rb.at[span(p)], ret.at[rows(e)], b_s.at[p], b_r.at[p], sp=e)

    def send_back(p):
        g = group(p)
        total = yp[g, local(p), cols(t)].astype(F32) + rc2[g, y, local(p)].astype(F32)
        for d in range(1, Y):
            y2_recv(p, yo(d)).wait_recv()
            total = total + ry2[g, yo(d), local(p)].astype(F32)
        if p:
            rb[span(p)] = total.astype(BF16)
            b_send(p).start()
        else:
            ret[rows(me)] = total.astype(BF16)

    def later(f, *args):
        return lambda: f(*args)

    arrivals = [Z] + list(range(1, Z))
    forward(0)
    due = [0]
    for i, p in enumerate(arrivals):
        arrive(p)
        due.append(p)
        if i:
            relay(due.pop(0))
    for p in far[:1]:
        arrive(p)
    while len(due) > 1:
        relay(due.pop(0))
    norm(0)
    for p in arrivals[:-1]:
        norm(p)
    relay(due.pop(0))
    for p in far[1:2]:
        arrive(p)
    norm(arrivals[-1])
    loads[9].wait()
    loads[10].wait()
    hidden(0, [later(arrive, p) for p in far[2:]] + [later(relay, p) for p in far[:2]])
    loads[11].wait()
    for p in far[2:]:
        relay(p)
    down(0)
    for p in far:
        norm(p)
    hidden(1, [])
    down(1)
    for p in back[0] + back[1]:
        send_back(p)

    for p in range(1, S):
        b_recv(p).wait_recv()

    mix0 = jnp.dot(picker(slot0).astype(BF16), ret[...], preferred_element_type=F32)
    mix1 = jnp.dot(picker(slot1).astype(BF16), ret[...], preferred_element_type=F32)
    o_all[:, cols(t)] = (
        mixed[...].astype(F32) + (column(rw[0:1, :]) * mix0 + column(rw[1:2, :]) * mix1)
    ).astype(BF16)

    def gy_send(yy):
        ref = o_all.at[:, cols(t)]
        return remote(ref, ref, gy_s.at[yy], gy_r.at[y], tp=tp_of(yy, c))

    def gy_recv(yy):
        ref = o_all.at[:, cols(tp_of(yy, c))]
        return remote(ref, ref, gy_s.at[yy], gy_r.at[yy], tp=tp_of(yy, c))

    def gc_send(yy):
        at = cols(tp_of(yy, c))
        return remote(
            o_all.at[:, at], out_hbm.at[:, at], gc_s.at[yy], gc_r.at[yy], tp=tp_of(y, oc)
        )

    def gc_recv(yy):
        at = cols(tp_of(yy, oc))
        return remote(
            o_all.at[:, at], out_hbm.at[:, at], gc_s.at[yy], gc_r.at[yy], tp=tp_of(y, oc)
        )

    def write(yy):
        at = cols(tp_of(yy, c))
        return pltpu.make_async_copy(o_all.at[:, at], out_hbm.at[:, at], o_sem.at[yy])

    for d in range(1, Y):
        gy_send(yo(d)).start()
    gc_send(y).start()
    write(y).start()
    for d in range(1, Y):
        gy_recv(yo(d)).wait_recv()
        gc_send(yo(d)).start()
        write(yo(d)).start()

    @pl.when(me < S - 1)
    def _():
        for copy in halo_copies:
            copy.wait_send()

    for d in range(Y):
        c1(yo(d)).wait_send()
        for g in range(2):
            c2(g, yo(d)).wait_send()
    for p in range(S):
        if p:
            for j in range(NH):
                a_send(p, j).wait_send()
            b_send(p).wait_send()
        for d in range(Y):
            fc_send(p, yo(d)).wait_send()
        for d in range(1, Y):
            fy_send(p, yo(d)).wait_send()
            y2_send(p, yo(d)).wait_send()
    for d in range(1, Y):
        for j in range(NH):
            y1_send(yo(d), j).wait_send()
        gy_send(yo(d)).wait_send()
    for d in range(Y):
        gc_recv(yo(d)).wait_recv()
        gc_send(yo(d)).wait_send()
        write(yo(d)).wait()


def per_device(
    S,
    T,
    queries,
    key_rows,
    value_rows,
    sink_logits,
    out_weight,
    residual,
    norm_gain,
    routes,
    route_weights,
    gate_weight,
    up_weight,
    down_weight,
):
    R, D = residual.shape
    HW = queries.shape[1]
    Y = T // CORES
    W = D // T
    C = 2 * R * TOP // S
    Z = S // 2
    M = (Z + 1) * C
    FL = gate_weight.shape[2]
    NH = 2 if W % 256 == 0 else 1
    hbm = pl.BlockSpec(memory_space=pl.ANY)
    dma = pltpu.SemaphoreType.DMA
    v = pltpu.VMEM
    return pl.pallas_call(
        functools.partial(kernel, S, T),
        out_shape=jax.ShapeDtypeStruct((R, D), BF16),
        in_specs=[hbm] * 12,
        out_specs=hbm,
        scratch_shapes=[
            v((1, sink_logits.shape[0]), F32),
            v(queries.shape, BF16),
            v(key_rows.shape, BF16),
            v(value_rows.shape, BF16),
            v((R, W), BF16),
            v((1, D), F32),
            v((TOP, R), jnp.int32),
            v((TOP, R), F32),
            v(out_weight.shape, BF16),
            v(gate_weight.shape[1:], BF16),
            v(up_weight.shape[1:], BF16),
            v(down_weight.shape[1:], BF16),
            v((2,) + key_rows.shape, BF16),
            v((R, HW), BF16),
            v((R, D), BF16),
            v((Y, R, W), BF16),
            v((Y, NH, R, W // NH), BF16),
            v((Y, NH, R, W // NH), BF16),
            v((R, W), BF16),
            v((S * C, W), BF16),
            v((S * C, D), BF16),
            v((S * C, D), BF16),
            v((M, FL), BF16),
            v((2, M, D), BF16),
            v((2, Y, M, W), BF16),
            v((2, Y, M, W), BF16),
            v((2, Y, M, W), BF16),
            v((S * C, W), BF16),
            v((S * C, W), BF16),
            v((R, D), BF16),
            dma((12,)),
            dma((2,)),
            dma((2,)),
            dma((Y,)),
            dma((Y,)),
            dma((Y, NH)),
            dma((Y, NH)),
            dma((S, NH)),
            dma((S, NH)),
            dma((S, Y)),
            dma((S, Y)),
            dma((S, Y)),
            dma((S, Y)),
            dma((2, Y)),
            dma((2, Y)),
            dma((S, Y)),
            dma((S, Y)),
            dma((S,)),
            dma((S,)),
            dma((Y,)),
            dma((Y,)),
            dma((Y,)),
            dma((Y,)),
            dma((Y,)),
        ],
        compiler_params=pltpu.CompilerParams(
            collective_id=0, has_side_effects=True, vmem_limit_bytes=60 * 1024 * 1024
        ),
        name="layer",
    )(
        sink_logits.reshape(1, -1),
        queries,
        key_rows,
        value_rows,
        residual,
        norm_gain.reshape(1, D),
        routes.T,
        route_weights.T,
        out_weight,
        gate_weight,
        up_weight,
        down_weight,
    )


def solution(mesh):
    placed = (
        P("sp", "tp"),
        P("sp", "tp"),
        P("sp", "tp"),
        P("tp"),
        P("tp", None),
        P("sp", None),
        P(),
        P("sp", None),
        P("sp", None),
        P("sp", None, "tp"),
        P("sp", None, "tp"),
        P("sp", "tp", None),
    )
    return jax.shard_map(
        functools.partial(per_device, mesh.shape["sp"], mesh.shape["tp"]),
        mesh=mesh,
        in_specs=placed,
        out_specs=P("sp", None),
        check_vma=False,
    )
```

```python
import functools

import jax
import jax.numpy as jnp
import numpy as np
from jax import lax
from jax.experimental import pallas as pl
from jax.experimental.pallas import tpu as pltpu
from jax.sharding import PartitionSpec as P

HEAD_DIM = 64
WINDOW = 128
TOP = 2
CORES = 2
F32 = jnp.float32
BF16 = jnp.bfloat16
MESH = pl.DeviceIdType.MESH


def kernel(
    S,
    T,
    sink_hbm,
    q_hbm,
    k_hbm,
    v_hbm,
    res_hbm,
    gain_hbm,
    routes_hbm,
    rw_hbm,
    wo_hbm,
    wg_hbm,
    wu_hbm,
    wd_hbm,
    out,
    sink,
    q,
    k,
    v,
    res,
    gain,
    routes,
    rw,
    wo,
    wg,
    wu,
    wd,
    halo,
    att,
    pp,
    rc1,
    sb1,
    ry1,
    mixed,
    picked,
    x_all,
    xn,
    act,
    yp,
    rc2,
    sb2,
    ry2,
    rb,
    ret,
    w_sem,
    sent,
    halo_r,
    c1_r,
    y1_r,
    a_r,
    fy_r,
    fc_r,
    c2_r,
    y2_r,
    b_r,
    gy_r,
    gc_r,
):
    R, W = res.shape
    D = W * T
    Y = T // CORES
    H = q.shape[1] // HEAD_DIM
    KV = k.shape[1] // HEAD_DIM
    G = H // KV
    C = x_all.shape[0] // S
    Z = S // 2
    NEAR = (Z + 1) * C
    FL = wg.shape[1]
    NH = y1_r.shape[1]
    HALO, C1, Y1, A, FY, FC, C2, Y2, B, GY, GC = (sent.at[i] for i in range(11))
    HW = W // NH

    me = lax.axis_index("sp")
    t = lax.axis_index("tp")
    y = t // CORES
    c = t % CORES
    oc = 1 - c
    z = me // 2
    x = me % 2

    def tp_of(yy, cc):
        return yy * CORES + cc

    def cols(tt):
        return pl.ds(pl.multiple_of(tt * W, W), W)

    def part(tt, j):
        return pl.ds(pl.multiple_of(tt * W + j * HW, HW), HW)

    def rows(s):
        return pl.ds(pl.multiple_of(s * C, C), C)

    def yo(d):
        return (y + d) % Y

    def seen(d):
        return Y - d - 1

    def remote(src, dst, ss, rs, **dev):
        return pltpu.make_async_remote_copy(
            src_ref=src, dst_ref=dst, send_sem=ss, recv_sem=rs, device_id=dev, device_id_type=MESH
        )

    def peer(p):
        zz = z
        bit = 1
        while bit < Z:
            if (p % Z) // bit % 2:
                zz = zz + bit * (1 - 2 * (zz // bit % 2))
            bit *= 2
        return 2 * zz + (x + p // Z) % 2

    far = list(range(Z + 1, 2 * Z))
    near = list(range(Z + 1))
    groups = ((0, near), (NEAR, far))

    def span(p):
        return pl.ds(p * C, C)

    def local(p):
        return pl.ds((p if p <= Z else p - Z - 1) * C, C)

    def group(p):
        return 0 if p <= Z else 1

    barrier = pltpu.get_barrier_semaphore()

    @pl.loop(1, S)
    def _(d):
        pl.semaphore_signal(
            barrier, inc=1, device_id={"sp": (me + d) % S}, device_id_type=MESH
        )

    for d in range(1, Y):
        pl.semaphore_signal(
            barrier, inc=1, device_id={"tp": tp_of(yo(d), c)}, device_id_type=MESH
        )
    pl.semaphore_signal(barrier, inc=1, device_id={"tp": tp_of(y, oc)}, device_id_type=MESH)

    loads = [
        pltpu.make_async_copy(src, dst, w_sem.at[i])
        for i, (src, dst) in enumerate(
            (
                (k_hbm, k),
                (v_hbm, v),
                (q_hbm, q),
                (routes_hbm, routes),
                (sink_hbm, sink),
                (res_hbm.at[:, cols(t)], res),
                (rw_hbm, rw),
                (gain_hbm, gain),
                (wo_hbm, wo),
                (wg_hbm.at[0], wg),
                (wu_hbm.at[0], wu),
                (wd_hbm.at[0], wd),
            )
        )
    ]
    for load in loads:
        load.start()
    loads[0].wait()
    loads[1].wait()
    pl.semaphore_wait(barrier, S - 1 + Y)

    halo_copies = [
        remote(src, halo.at[i], HALO, halo_r.at[i], sp=jnp.minimum(me + 1, S - 1))
        for i, src in enumerate((k, v))
    ]

    @pl.when(me < S - 1)
    def _():
        for copy in halo_copies:
            copy.start()

    for load in loads[2:5]:
        load.wait()

    qi = lax.broadcasted_iota(jnp.int32, (R, R), 0)
    kj = lax.broadcasted_iota(jnp.int32, (R, R), 1)
    dist_own = (qi - kj).astype(F32)
    dist_old = (qi - kj + WINDOW).astype(F32)
    nt = (((1,), (1,)), ((), ()))

    ok_own = qi >= kj
    ok_old = (kj >= qi) & (kj + me * R >= WINDOW)

    base = jnp.float32(1.0)
    for i in range(1, T):
        base = jnp.where(t == i, jnp.float32(2.0 ** (-8.0 * i / T)), base)

    def head(h):
        return slice(h * HEAD_DIM, (h + 1) * HEAD_DIM), slice(
            (h // G) * HEAD_DIM, (h // G + 1) * HEAD_DIM
        )

    def scores(h, keys, dist, ok):
        raw = lax.dot_general(q[:, head(h)[0]], keys, nt, preferred_element_type=F32)
        slope = base * np.float32(2.0 ** (-8.0 * (h + 1) / (H * T)))
        return jnp.where(ok, raw * HEAD_DIM**-0.5 - slope * dist, -jnp.inf)

    s_own = [scores(h, k[:, head(h)[1]], dist_own, ok_own) for h in range(H)]
    top = [jnp.max(a, axis=1, keepdims=True) for a in s_own]
    e_own = [jnp.exp(a - b) for a, b in zip(s_own, top)]
    weight = [jnp.sum(a, axis=1, keepdims=True) for a in e_own]
    mix_own = [
        jnp.dot(a.astype(BF16), v[:, head(h)[1]], preferred_element_type=F32)
        for h, a in enumerate(e_own)
    ]

    def column(row):
        return jnp.broadcast_to(row, (R, R)).T[:, 0:1]

    r0 = column(routes[0:1, :].astype(F32)).astype(jnp.int32)
    r1 = column(routes[1:2, :].astype(F32)).astype(jnp.int32)
    lane_e = lax.broadcasted_iota(jnp.int32, (R, 128), 1)
    hit0 = lane_e == r0
    hit1 = lane_e == r1
    member = jnp.where(hit0 | hit1, 1.0, 0.0).astype(BF16)
    tri = jnp.where(
        lax.broadcasted_iota(jnp.int32, (R, R), 1) < lax.broadcasted_iota(jnp.int32, (R, R), 0),
        1.0,
        0.0,
    ).astype(BF16)
    rank = jnp.dot(tri, member, preferred_element_type=F32)
    rank0 = jnp.sum(jnp.where(hit0, rank, 0.0), axis=1, keepdims=True)
    rank1 = jnp.sum(jnp.where(hit1, rank, 0.0), axis=1, keepdims=True)
    slot0 = r0.astype(F32) * C + rank0
    slot1 = r1.astype(F32) * C + rank1
    lane_s = lax.broadcasted_iota(jnp.int32, (R, S * C), 1).astype(F32)

    def picker(slot):
        return jnp.where(lane_s == slot, 1.0, 0.0)

    both = (picker(slot0) + picker(slot1)).T.astype(BF16)

    @pl.when(me > 0)
    def _():
        halo_copies[0].wait_recv()

    @pl.when(me == 0)
    def _():
        halo[...] = jnp.zeros_like(halo)

    s_old = [scores(h, halo[0, :, head(h)[1]], dist_old, ok_old) for h in range(H)]
    peak = [jnp.maximum(a, jnp.max(b, axis=1, keepdims=True)) for a, b in zip(top, s_old)]
    shrink = [jnp.exp(a - b) for a, b in zip(top, peak)]
    e_old = [jnp.exp(a - b) for a, b in zip(s_old, peak)]
    total = [
        a * b + jnp.sum(e, axis=1, keepdims=True) for a, b, e in zip(weight, shrink, e_old)
    ]
    keep = [
        1.0 / (a + jnp.exp(sink[0:1, h : h + 1] - b)) for h, (a, b) in enumerate(zip(total, peak))
    ]

    @pl.when(me > 0)
    def _():
        halo_copies[1].wait_recv()

    mix_old = [
        jnp.dot(a.astype(BF16), halo[1, :, head(h)[1]], preferred_element_type=F32)
        for h, a in enumerate(e_old)
    ]
    for h in range(H):
        att[:, head(h)[0]] = ((mix_own[h] * shrink[h] + mix_old[h]) * keep[h]).astype(BF16)

    for load in loads[5:9]:
        load.wait()

    def project(tt):
        pp[:, cols(tt)] = jnp.dot(att[...], wo[:, cols(tt)], preferred_element_type=F32).astype(
            BF16
        )

    def c1(yy):
        return remote(
            pp.at[:, cols(tp_of(yy, oc))], rc1.at[yy], C1, c1_r.at[yy], tp=tp_of(y, oc)
        )

    def y1_send(d, j):
        yy = yo(d)
        return remote(
            sb1.at[yy, j], ry1.at[y, j], Y1, y1_r.at[seen(d), j], tp=tp_of(yy, c)
        )

    def y1_recv(d, j):
        yy = yo(d)
        return remote(sb1.at[yy, j], ry1.at[yy, j], Y1, y1_r.at[d - 1, j], tp=tp_of(yy, c))

    turns = list(range(1, Y)) + [0]

    def half(j):
        return slice(j * HW, (j + 1) * HW)

    for d in turns:
        project(tp_of(yo(d), oc))
        c1(yo(d)).start()
    for d in turns:
        project(tp_of(yo(d), c))
    for d in range(1, Y):
        c1(yo(d)).wait_recv()
        for j in range(NH):
            sb1[yo(d), j] = (
                pp[:, part(tp_of(yo(d), c), j)].astype(F32) + rc1[yo(d), :, half(j)].astype(F32)
            ).astype(BF16)
            y1_send(d, j).start()
    c1(y).wait_recv()

    def a_send(p, j):
        e = peer(p)
        return remote(
            picked.at[rows(e), half(j)], x_all.at[span(p), part(t, j)], A, a_r.at[p], sp=e
        )

    def a_recv(p):
        e = peer(p)
        return remote(picked.at[rows(e)], x_all.at[span(p), cols(t)], A, a_r.at[p], sp=e)

    def fy_send(p, d):
        ref = x_all.at[span(p), cols(t)]
        return remote(ref, ref, FY, fy_r.at[p, seen(d)], tp=tp_of(yo(d), c))

    def fy_recv(p, d):
        ref = x_all.at[span(p), cols(tp_of(yo(d), c))]
        return remote(ref, ref, FY, fy_r.at[p, d - 1], tp=tp_of(yo(d), c))

    def fc_send(p, d):
        ref = x_all.at[span(p), cols(tp_of(yo(d), c))]
        return remote(ref, ref, FC, fc_r.at[p], tp=tp_of(y, oc))

    def fc_recv(p):
        ref = x_all.at[span(p), pl.ds(0, Y * W)]
        return remote(ref, ref, FC, fc_r.at[p], tp=tp_of(y, oc))

    arrivals = [Z] + list(range(1, Z))

    for j in range(NH):
        head_sum = pp[:, part(t, j)].astype(F32) + rc1[y, :, half(j)].astype(F32)
        for d in range(1, Y):
            y1_recv(d, j).wait_recv()
            head_sum = head_sum + ry1[yo(d), j].astype(F32)
        mixed[:, half(j)] = (res[:, half(j)].astype(F32) + head_sum).astype(BF16)
        picked[:, half(j)] = jnp.dot(
            both, mixed[:, half(j)], preferred_element_type=F32
        ).astype(BF16)
        for p in arrivals:
            a_send(p, j).start()
    x_all[span(0), cols(t)] = picked[rows(me)]

    def forward(p):
        for d in range(1, Y):
            fy_send(p, d).start()
        fc_send(p, 0).start()

    def relay(p):
        for d in range(1, Y):
            fy_recv(p, d).wait_recv()
            fc_send(p, d).start()

    def arrive(p):
        a_recv(p).wait_recv()
        forward(p)

    def norm(p):
        fc_recv(p).wait_recv()
        wide = x_all[span(p)].astype(F32)
        scale = lax.rsqrt(jnp.mean(wide * wide, axis=1, keepdims=True) + 1e-06)
        xn[span(p)] = (wide * scale * gain[...]).astype(BF16)

    TN = min(256, FL)
    NT = FL // TN

    def hidden(g, hooks):
        first, places = groups[g]
        m = len(places) * C

        @pl.loop(0, NT)
        def _(n):
            nn = pl.ds(pl.multiple_of(n * TN, TN), TN)
            gate = jnp.dot(xn[first : first + m], wg[:, nn], preferred_element_type=F32)
            up = jnp.dot(xn[first : first + m], wu[:, nn], preferred_element_type=F32)
            act[0:m, nn] = (gate / (1.0 + jnp.exp(-gate)) * up).astype(BF16)
            for i in range(NT):
                todo = hooks[i * len(hooks) // NT : (i + 1) * len(hooks) // NT]
                if todo:

                    @pl.when(n == i)
                    def _(todo=todo):
                        for hook in todo:
                            hook()

    def c2(g, yy):
        m = len(groups[g][1]) * C
        return remote(
            yp.at[g, pl.ds(0, m), cols(tp_of(yy, oc))],
            rc2.at[g, yy, pl.ds(0, m)],
            C2,
            c2_r.at[g, yy],
            tp=tp_of(y, oc),
        )

    def down_block(g, tt):
        m = len(groups[g][1]) * C
        yp[g, 0:m, cols(tt)] = jnp.dot(
            act[0:m], wd[:, cols(tt)], preferred_element_type=F32
        ).astype(BF16)

    def y2_send(p, d):
        g, yy = group(p), yo(d)
        return remote(
            sb2.at[g, yy, local(p)],
            ry2.at[g, y, local(p)],
            Y2,
            y2_r.at[p, seen(d)],
            tp=tp_of(yy, c),
        )

    def y2_recv(p, d):
        g, yy = group(p), yo(d)
        return remote(
            sb2.at[g, yy, local(p)], ry2.at[g, yy, local(p)], Y2, y2_r.at[p, d - 1], tp=tp_of(yy, c)
        )

    back = (list(range(2, Z)) + [1, Z, 0], far[1:] + far[:1])

    def pair_sum(g, d):
        yy = yo(d)
        c2(g, yy).wait_recv()
        for p in back[g]:
            sb2[g, yy, local(p)] = (
                yp[g, local(p), cols(tp_of(yy, c))].astype(F32)
                + rc2[g, yy, local(p)].astype(F32)
            ).astype(BF16)
            if p:
                y2_send(p, d).start()

    def down(g):
        held = None
        for d in turns:
            down_block(g, tp_of(yo(d), oc))
            c2(g, yo(d)).start()
            if held is not None:
                pair_sum(g, held)
            down_block(g, tp_of(yo(d), c))
            held = d
        c2(g, y).wait_recv()

    def b_send(p):
        e = peer(p)
        return remote(rb.at[span(p)], ret.at[rows(me)], B, b_r.at[0], sp=e)

    def send_back(p):
        g = group(p)
        total = yp[g, local(p), cols(t)].astype(F32) + rc2[g, y, local(p)].astype(F32)
        for d in range(1, Y):
            y2_recv(p, d).wait_recv()
            total = total + ry2[g, yo(d), local(p)].astype(F32)
        if p:
            rb[span(p)] = total.astype(BF16)
            b_send(p).start()
        else:
            ret[rows(me)] = total.astype(BF16)

    def later(f, *args):
        return lambda: f(*args)

    forward(0)
    due = [0]
    for i, p in enumerate(arrivals):
        arrive(p)
        due.append(p)
        if i == 0:
            for f in far:
                for j in range(NH):
                    a_send(f, j).start()
        else:
            relay(due.pop(0))
    for p in far[:1]:
        arrive(p)
    while len(due) > 1:
        relay(due.pop(0))
    norm(0)
    for p in arrivals[:-1]:
        norm(p)
    relay(due.pop(0))
    for p in far[1:2]:
        arrive(p)
    norm(arrivals[-1])
    loads[9].wait()
    loads[10].wait()
    hidden(0, [later(arrive, p) for p in far[2:]] + [later(relay, p) for p in far[:2]])
    loads[11].wait()
    for p in far[2:]:
        relay(p)
    down(0)
    for p in far:
        norm(p)
    hidden(1, [])
    down(1)
    for d in range(1, Y):
        y2_send(0, d).start()
    for p in back[0][:-1] + back[1] + [0]:
        send_back(p)

    others = pl.ds(0, (S - 1) * C)
    remote(rb.at[others], ret.at[others], B, b_r.at[0], sp=peer(1)).wait_recv()

    def gy_send(d, j):
        ref = out.at[:, part(t, j)]
        return remote(ref, ref, GY, gy_r.at[seen(d), j], tp=tp_of(yo(d), c))

    def gy_recv(d, j):
        ref = out.at[:, part(tp_of(yo(d), c), j)]
        return remote(ref, ref, GY, gy_r.at[d - 1, j], tp=tp_of(yo(d), c))

    def gc_send(d, j):
        ref = out.at[:, part(tp_of(yo(d), c), j)]
        return remote(ref, ref, GC, gc_r.at[0], tp=tp_of(y, oc))

    pick0 = picker(slot0).astype(BF16)
    pick1 = picker(slot1).astype(BF16)
    rw0 = column(rw[0:1, :])
    rw1 = column(rw[1:2, :])
    for j in range(NH):
        mix0 = jnp.dot(pick0, ret[:, half(j)], preferred_element_type=F32)
        mix1 = jnp.dot(pick1, ret[:, half(j)], preferred_element_type=F32)
        out[:, part(t, j)] = (
            mixed[:, half(j)].astype(F32) + (rw0 * mix0 + rw1 * mix1)
        ).astype(BF16)
        for d in range(1, Y):
            gy_send(d, j).start()
        gc_send(0, j).start()

    @pl.when(me < S - 1)
    def _():
        remote(halo, halo, HALO, halo_r.at[0], sp=me + 1).wait_send()

    def drain(ref, sem):
        remote(ref, ref, sem, sem, tp=tp_of(y, oc)).wait_send()

    drain(rc1, C1)
    drain(sb1.at[pl.ds(0, Y - 1)], Y1)
    drain(ret.at[others], A)
    drain(x_all.at[:, pl.ds(0, (Y - 1) * W)], FY)
    drain(x_all.at[:, pl.ds(0, Y * W)], FC)
    drain(x_all.at[:, pl.ds(0, Y * W)], C2)
    drain(x_all.at[:, pl.ds(0, (Y - 1) * W)], Y2)
    drain(ret.at[others], B)

    for j in range(NH):
        for d in range(1, Y):
            gy_recv(d, j).wait_recv()
            gc_send(d, j).start()
    ours = out.at[:, pl.ds(0, Y * W)]
    remote(ours, ours, GC, gc_r.at[0], tp=tp_of(y, oc)).wait_recv()
    drain(ours, GC)
    drain(out.at[:, pl.ds(0, (Y - 1) * W)], GY)


def per_device(
    S,
    T,
    queries,
    key_rows,
    value_rows,
    sink_logits,
    out_weight,
    residual,
    norm_gain,
    routes,
    route_weights,
    gate_weight,
    up_weight,
    down_weight,
):
    R, D = residual.shape
    HW = queries.shape[1]
    Y = T // CORES
    W = D // T
    C = 2 * R * TOP // S
    Z = S // 2
    M = (Z + 1) * C
    FL = gate_weight.shape[2]
    NH = 2 if W % 256 == 0 else 1
    hbm = pl.BlockSpec(memory_space=pl.ANY)
    dma = pltpu.SemaphoreType.DMA
    v = pltpu.VMEM
    return pl.pallas_call(
        functools.partial(kernel, S, T),
        out_shape=v((R, D), BF16),
        in_specs=[hbm] * 12,
        out_specs=pl.BlockSpec(memory_space=v),
        scratch_shapes=[
            v((1, sink_logits.shape[0]), F32),
            v(queries.shape, BF16),
            v(key_rows.shape, BF16),
            v(value_rows.shape, BF16),
            v((R, W), BF16),
            v((1, D), F32),
            v((TOP, R), jnp.int32),
            v((TOP, R), F32),
            v(out_weight.shape, BF16),
            v(gate_weight.shape[1:], BF16),
            v(up_weight.shape[1:], BF16),
            v(down_weight.shape[1:], BF16),
            v((2,) + key_rows.shape, BF16),
            v((R, HW), BF16),
            v((R, D), BF16),
            v((Y, R, W), BF16),
            v((Y, NH, R, W // NH), BF16),
            v((Y, NH, R, W // NH), BF16),
            v((R, W), BF16),
            v((S * C, W), BF16),
            v((S * C, D), BF16),
            v((S * C, D), BF16),
            v((M, FL), BF16),
            v((2, M, D), BF16),
            v((2, Y, M, W), BF16),
            v((2, Y, M, W), BF16),
            v((2, Y, M, W), BF16),
            v((S * C, W), BF16),
            v((S * C, W), BF16),
            dma((12,)),
            dma((11,)),
            dma((2,)),
            dma((Y,)),
            dma((Y - 1, NH)),
            dma((S,)),
            dma((S, Y - 1)),
            dma((S,)),
            dma((2, Y)),
            dma((S, Y - 1)),
            dma((1,)),
            dma((Y - 1, NH)),
            dma((1,)),
        ],
        compiler_params=pltpu.CompilerParams(
            collective_id=0, has_side_effects=True, vmem_limit_bytes=60 * 1024 * 1024
        ),
        name="layer",
    )(
        sink_logits.reshape(1, -1),
        queries,
        key_rows,
        value_rows,
        residual,
        norm_gain.reshape(1, D),
        routes.T,
        route_weights.T,
        out_weight,
        gate_weight,
        up_weight,
        down_weight,
    )


def solution(mesh):
    placed = (
        P("sp", "tp"),
        P("sp", "tp"),
        P("sp", "tp"),
        P("tp"),
        P("tp", None),
        P("sp", None),
        P(),
        P("sp", None),
        P("sp", None),
        P("sp", None, "tp"),
        P("sp", None, "tp"),
        P("sp", "tp", None),
    )
    return jax.shard_map(
        functools.partial(per_device, mesh.shape["sp"], mesh.shape["tp"]),
        mesh=mesh,
        in_specs=placed,
        out_specs=P("sp", None),
        check_vma=False,
    )
```

```python
import functools

import jax
import jax.numpy as jnp
import numpy as np
from jax import lax
from jax.experimental import pallas as pl
from jax.experimental.pallas import tpu as pltpu
from jax.sharding import PartitionSpec as P

HEAD_DIM = 64
WINDOW = 128
TOP = 2
CORES = 2
F32 = jnp.float32
BF16 = jnp.bfloat16
MESH = pl.DeviceIdType.MESH


def kernel(
    S,
    T,
    sink_hbm,
    q_hbm,
    k_hbm,
    v_hbm,
    res_hbm,
    gain_hbm,
    routes_hbm,
    rw_hbm,
    wo_hbm,
    wg_hbm,
    wu_hbm,
    wd_hbm,
    out,
    sink,
    q,
    k,
    v,
    res,
    gain,
    routes,
    rw,
    wo,
    wg,
    wu,
    wd,
    halo,
    att,
    pp,
    rc1,
    sb1,
    ry1,
    mixed,
    picked,
    x_all,
    xn,
    act,
    yp,
    rc2,
    sb2,
    ry2,
    rb,
    ret,
    w_sem,
    sent,
    halo_r,
    c1_r,
    y1_r,
    a_r,
    fy_r,
    fc_r,
    c2_r,
    y2_r,
    b_r,
    gy_r,
    gc_r,
):
    R, W = res.shape
    D = W * T
    Y = T // CORES
    H = q.shape[1] // HEAD_DIM
    KV = k.shape[1] // HEAD_DIM
    G = H // KV
    C = x_all.shape[0] // S
    Z = S // 2
    FL = wg.shape[1]
    NH = y1_r.shape[1]
    HALO, C1, Y1, A, FY, FC, C2, Y2, B, GY, GC = (sent.at[i] for i in range(11))
    HW = W // NH
    NF = gy_r.shape[1]
    FW = W // NF

    me = lax.axis_index("sp")
    t = lax.axis_index("tp")
    y = t // CORES
    c = t % CORES
    oc = 1 - c
    z = me // 2
    x = me % 2

    def tp_of(yy, cc):
        return yy * CORES + cc

    def cols(tt):
        return pl.ds(pl.multiple_of(tt * W, W), W)

    def part(tt, j):
        return pl.ds(pl.multiple_of(tt * W + j * HW, HW), HW)

    def wide(tt, f):
        return pl.ds(pl.multiple_of(tt * W + f * FW, FW), FW)

    def fold(f):
        return pl.ds(f * FW, FW)

    def rows(s):
        return pl.ds(pl.multiple_of(s * C, C), C)

    def yo(d):
        return (y + d) % Y

    def seen(d):
        return Y - d - 1

    def remote(src, dst, ss, rs, **dev):
        return pltpu.make_async_remote_copy(
            src_ref=src, dst_ref=dst, send_sem=ss, recv_sem=rs, device_id=dev, device_id_type=MESH
        )

    places = [(0, 0), (1, 0)] + [(0, d) for d in range(1, Z)] + [(1, d) for d in range(1, Z)]
    split = min(3, Z + 1)
    first = list(range(split))
    second = list(range(split, Z + 1))
    third = list(range(Z + 1, S))

    def peer(p):
        parity, bits = places[p]
        zz = z
        bit = 1
        while bit < Z:
            if bits // bit % 2:
                zz = zz + bit * (1 - 2 * (zz // bit % 2))
            bit *= 2
        return 2 * zz + (x + parity) % 2

    def span(p):
        return pl.ds(p * C, C)

    def block(group):
        return pl.ds(group[0] * C, len(group) * C)

    barrier = pltpu.get_barrier_semaphore()

    @pl.loop(1, S)
    def _(d):
        pl.semaphore_signal(
            barrier, inc=1, device_id={"sp": (me + d) % S}, device_id_type=MESH
        )

    for d in range(1, Y):
        pl.semaphore_signal(
            barrier, inc=1, device_id={"tp": tp_of(yo(d), c)}, device_id_type=MESH
        )
    pl.semaphore_signal(barrier, inc=1, device_id={"tp": tp_of(y, oc)}, device_id_type=MESH)

    loads = [
        pltpu.make_async_copy(src, dst, w_sem.at[i])
        for i, (src, dst) in enumerate(
            (
                (k_hbm, k),
                (v_hbm, v),
                (q_hbm, q),
                (routes_hbm, routes),
                (sink_hbm, sink),
                (res_hbm.at[:, cols(t)], res),
                (rw_hbm, rw),
                (gain_hbm, gain),
                (wo_hbm, wo),
                (wg_hbm.at[0], wg),
                (wu_hbm.at[0], wu),
                (wd_hbm.at[0], wd),
            )
        )
    ]
    for load in loads:
        load.start()
    loads[0].wait()
    loads[1].wait()
    pl.semaphore_wait(barrier, S - 1 + Y)

    halo_copies = [
        remote(src, halo.at[i], HALO, halo_r.at[i], sp=jnp.minimum(me + 1, S - 1))
        for i, src in enumerate((k, v))
    ]

    @pl.when(me < S - 1)
    def _():
        for copy in halo_copies:
            copy.start()

    for load in loads[2:5]:
        load.wait()

    qi = lax.broadcasted_iota(jnp.int32, (R, R), 0)
    kj = lax.broadcasted_iota(jnp.int32, (R, R), 1)
    dist_own = (qi - kj).astype(F32)
    dist_old = (qi - kj + WINDOW).astype(F32)
    nt = (((1,), (1,)), ((), ()))

    ok_own = qi >= kj
    ok_old = (kj >= qi) & (kj + me * R >= WINDOW)

    base = jnp.float32(1.0)
    for i in range(1, T):
        base = jnp.where(t == i, jnp.float32(2.0 ** (-8.0 * i / T)), base)

    def head(h):
        return slice(h * HEAD_DIM, (h + 1) * HEAD_DIM), slice(
            (h // G) * HEAD_DIM, (h // G + 1) * HEAD_DIM
        )

    def scores(h, keys, dist, ok):
        raw = lax.dot_general(q[:, head(h)[0]], keys, nt, preferred_element_type=F32)
        slope = base * np.float32(2.0 ** (-8.0 * (h + 1) / (H * T)))
        return jnp.where(ok, raw * HEAD_DIM**-0.5 - slope * dist, -jnp.inf)

    s_own = [scores(h, k[:, head(h)[1]], dist_own, ok_own) for h in range(H)]
    top = [jnp.max(a, axis=1, keepdims=True) for a in s_own]
    e_own = [jnp.exp(a - b) for a, b in zip(s_own, top)]
    weight = [jnp.sum(a, axis=1, keepdims=True) for a in e_own]
    mix_own = [
        jnp.dot(a.astype(BF16), v[:, head(h)[1]], preferred_element_type=F32)
        for h, a in enumerate(e_own)
    ]

    def column(row):
        return jnp.broadcast_to(row, (R, R)).T[:, 0:1]

    r0 = column(routes[0:1, :].astype(F32)).astype(jnp.int32)
    r1 = column(routes[1:2, :].astype(F32)).astype(jnp.int32)
    lane_e = lax.broadcasted_iota(jnp.int32, (R, 128), 1)
    hit0 = lane_e == r0
    hit1 = lane_e == r1
    member = jnp.where(hit0 | hit1, 1.0, 0.0).astype(BF16)
    tri = jnp.where(
        lax.broadcasted_iota(jnp.int32, (R, R), 1) < lax.broadcasted_iota(jnp.int32, (R, R), 0),
        1.0,
        0.0,
    ).astype(BF16)
    rank = jnp.dot(tri, member, preferred_element_type=F32)
    rank0 = jnp.sum(jnp.where(hit0, rank, 0.0), axis=1, keepdims=True)
    rank1 = jnp.sum(jnp.where(hit1, rank, 0.0), axis=1, keepdims=True)
    slot0 = r0.astype(F32) * C + rank0
    slot1 = r1.astype(F32) * C + rank1
    lane_s = lax.broadcasted_iota(jnp.int32, (R, S * C), 1).astype(F32)

    def picker(slot):
        return jnp.where(lane_s == slot, 1.0, 0.0)

    both = (picker(slot0) + picker(slot1)).T.astype(BF16)

    @pl.when(me > 0)
    def _():
        halo_copies[0].wait_recv()

    @pl.when(me == 0)
    def _():
        halo[...] = jnp.zeros_like(halo)

    s_old = [scores(h, halo[0, :, head(h)[1]], dist_old, ok_old) for h in range(H)]
    peak = [jnp.maximum(a, jnp.max(b, axis=1, keepdims=True)) for a, b in zip(top, s_old)]
    shrink = [jnp.exp(a - b) for a, b in zip(top, peak)]
    e_old = [jnp.exp(a - b) for a, b in zip(s_old, peak)]
    total = [
        a * b + jnp.sum(e, axis=1, keepdims=True) for a, b, e in zip(weight, shrink, e_old)
    ]
    keep = [
        1.0 / (a + jnp.exp(sink[0:1, h : h + 1] - b)) for h, (a, b) in enumerate(zip(total, peak))
    ]

    @pl.when(me > 0)
    def _():
        halo_copies[1].wait_recv()

    mix_old = [
        jnp.dot(a.astype(BF16), halo[1, :, head(h)[1]], preferred_element_type=F32)
        for h, a in enumerate(e_old)
    ]
    for h in range(H):
        att[:, head(h)[0]] = ((mix_own[h] * shrink[h] + mix_old[h]) * keep[h]).astype(BF16)

    for load in loads[5:9]:
        load.wait()

    def project(tt):
        pp[:, cols(tt)] = jnp.dot(att[...], wo[:, cols(tt)], preferred_element_type=F32).astype(
            BF16
        )

    def c1(yy):
        return remote(
            pp.at[:, cols(tp_of(yy, oc))], rc1.at[yy], C1, c1_r.at[yy], tp=tp_of(y, oc)
        )

    def y1_send(d, j):
        yy = yo(d)
        return remote(
            sb1.at[yy, j], ry1.at[y, j], Y1, y1_r.at[seen(d), j], tp=tp_of(yy, c)
        )

    def y1_recv(d, j):
        yy = yo(d)
        return remote(sb1.at[yy, j], ry1.at[yy, j], Y1, y1_r.at[d - 1, j], tp=tp_of(yy, c))

    turns = list(range(1, Y)) + [0]

    def half(j):
        return slice(j * HW, (j + 1) * HW)

    for d in turns:
        project(tp_of(yo(d), oc))
        c1(yo(d)).start()
    for d in turns:
        project(tp_of(yo(d), c))
    for d in range(1, Y):
        c1(yo(d)).wait_recv()
        for j in range(NH):
            sb1[yo(d), j] = (
                pp[:, part(tp_of(yo(d), c), j)].astype(F32) + rc1[yo(d), :, half(j)].astype(F32)
            ).astype(BF16)
            y1_send(d, j).start()
    c1(y).wait_recv()

    def a_send(p, j):
        e = peer(p)
        return remote(
            picked.at[rows(e), half(j)],
            x_all.at[span(p), part(t, j)],
            A,
            a_r.at[p, j * NF // NH],
            sp=e,
        )

    def a_fold(p, f):
        e = peer(p)
        return remote(
            picked.at[rows(e), fold(f)], x_all.at[span(p), wide(t, f)], A, a_r.at[p, f], sp=e
        )

    def fy_send(p, d, f):
        ref = x_all.at[span(p), wide(t, f)]
        return remote(ref, ref, FY, fy_r.at[p, seen(d), f], tp=tp_of(yo(d), c))

    def fy_recv(p, d, f):
        ref = x_all.at[span(p), wide(tp_of(yo(d), c), f)]
        return remote(ref, ref, FY, fy_r.at[p, d - 1, f], tp=tp_of(yo(d), c))

    def fc_send(p, d, f):
        ref = x_all.at[span(p), wide(tp_of(yo(d), c), f)]
        return remote(ref, ref, FC, fc_r.at[p], tp=tp_of(y, oc))

    def fc_recv(p):
        ref = x_all.at[span(p), pl.ds(0, Y * W)]
        return remote(ref, ref, FC, fc_r.at[p], tp=tp_of(y, oc))

    arrivals = list(range(1, Z + 1))

    for j in range(NH):
        head_sum = pp[:, part(t, j)].astype(F32) + rc1[y, :, half(j)].astype(F32)
        for d in range(1, Y):
            y1_recv(d, j).wait_recv()
            head_sum = head_sum + ry1[yo(d), j].astype(F32)
        mixed[:, half(j)] = (res[:, half(j)].astype(F32) + head_sum).astype(BF16)
        picked[:, half(j)] = jnp.dot(
            both, mixed[:, half(j)], preferred_element_type=F32
        ).astype(BF16)
        for p in arrivals:
            a_send(p, j).start()
    x_all[span(0), cols(t)] = picked[rows(me)]

    def forward(p, f):
        for d in range(1, Y):
            fy_send(p, d, f).start()
        fc_send(p, 0, f).start()

    def relay(p):
        for f in range(NF):
            for d in range(1, Y):
                fy_recv(p, d, f).wait_recv()
                fc_send(p, d, f).start()

    def arrive(p):
        for f in range(NF):
            a_fold(p, f).wait_recv()
            forward(p, f)

    def norm(p):
        fc_recv(p).wait_recv()
        wide = x_all[span(p)].astype(F32)
        scale = lax.rsqrt(jnp.mean(wide * wide, axis=1, keepdims=True) + 1e-06)
        xn[span(p)] = (wide * scale * gain[...]).astype(BF16)

    TN = min(256, FL)
    NT = FL // TN

    def hidden(group, hooks):
        at = block(group)

        @pl.loop(0, NT)
        def _(n):
            nn = pl.ds(pl.multiple_of(n * TN, TN), TN)
            gate = jnp.dot(xn[at], wg[:, nn], preferred_element_type=F32)
            up = jnp.dot(xn[at], wu[:, nn], preferred_element_type=F32)
            act[at, nn] = (gate / (1.0 + jnp.exp(-gate)) * up).astype(BF16)
            for i in range(NT):
                todo = [hook for turn, hook in hooks if min(turn, NT - 1) == i]
                if todo:

                    @pl.when(n == i)
                    def _(todo=todo):
                        for hook in todo:
                            hook()

    def c2(g, d):
        at = block(groups[g])
        return remote(
            yp.at[at, cols(tp_of(yo(d), oc))], rc2.at[d, at], C2, c2_r.at[g, d], tp=tp_of(y, oc)
        )

    def down_block(g, tt):
        at = block(groups[g])
        yp[at, cols(tt)] = jnp.dot(act[at], wd[:, cols(tt)], preferred_element_type=F32).astype(
            BF16
        )

    def y2_send(p, d, f):
        return remote(
            sb2.at[d - 1, span(p), fold(f)],
            ry2.at[seen(d), span(p), fold(f)],
            Y2,
            y2_r.at[p, seen(d), f],
            tp=tp_of(yo(d), c),
        )

    def y2_recv(p, d, f):
        return remote(
            sb2.at[d - 1, span(p), fold(f)],
            ry2.at[d - 1, span(p), fold(f)],
            Y2,
            y2_r.at[p, d - 1, f],
            tp=tp_of(yo(d), c),
        )

    groups = [g for g in (first, second, third) if g]
    back = [g[:0:-1] + g[:1] if g is first else g[1:] + g[:1] for g in groups]

    def pair_sum(g, d):
        c2(g, d).wait_recv()
        for p in back[g]:
            at = span(p)
            sb2[d - 1, at] = (
                yp[at, cols(tp_of(yo(d), c))].astype(F32) + rc2[d, at].astype(F32)
            ).astype(BF16)
            for f in range(NF):
                y2_send(p, d, f).start()

    def down(g, hooks):
        held = None
        hooks = list(hooks)
        for d in turns:
            down_block(g, tp_of(yo(d), oc))
            c2(g, d).start()
            if held is not None:
                pair_sum(g, held)
            if hooks:
                hooks.pop(0)()
            down_block(g, tp_of(yo(d), c))
            if hooks:
                hooks.pop(0)()
            held = d or None
        for hook in hooks:
            hook()
        c2(g, 0).wait_recv()

    def b_send(p, f):
        e = peer(p)
        return remote(
            rb.at[span(p), fold(f)], ret.at[rows(me), fold(f)], B, b_r.at[0], sp=e
        )

    def send_back(p):
        at = span(p)
        for f in range(NF):
            total = yp[at, wide(t, f)].astype(F32) + rc2[0, at, fold(f)].astype(F32)
            for d in range(1, Y):
                y2_recv(p, d, f).wait_recv()
                total = total + ry2[d - 1, at, fold(f)].astype(F32)
            if p:
                rb[at, fold(f)] = total.astype(BF16)
                b_send(p, f).start()
            else:
                ret[rows(me), fold(f)] = total.astype(BF16)

    def later(f, *args):
        return lambda: f(*args)

    for f in range(NF):
        forward(0, f)
    for i, p in enumerate(arrivals):
        arrive(p)
        if i == 0:
            for q in third:
                for f in range(NF):
                    a_fold(q, f).start()
        elif p <= split:
            relay(p - 2)
    for p in range(min(split, Z) - 1, split):
        relay(p)
    for p in first:
        norm(p)
    loads[9].wait()
    loads[10].wait()
    steps = [later(arrive, p) for p in third[:1]] + [later(relay, p) for p in second]
    steps += [later(arrive, p) for p in third[1:2]]
    hidden(first, [(i, step) for i, step in enumerate(steps)])
    loads[11].wait()
    if second:
        for p in second:
            norm(p)
        steps = [later(arrive, p) for p in third[2:]] + [later(relay, p) for p in third[:-2]]
        hidden(second, [(i, step) for i, step in enumerate(steps)])
        down(1, [later(lambda: None), later(relay, third[-2])])
    else:
        for p in third[2:]:
            arrive(p)
        for p in third[:-1]:
            relay(p)
    down(0, [later(lambda: None), later(relay, third[-1])])
    for p in third:
        norm(p)
    steps = [later(send_back, p) for p in back[1]] if second else []
    hidden(third, [(2 * i + 1, step) for i, step in enumerate(steps)])
    down(len(groups) - 1, [])
    for p in back[0] + back[-1]:
        send_back(p)

    others = pl.ds(0, (S - 1) * C)
    remote(rb.at[others], ret.at[others], B, b_r.at[0], sp=peer(1)).wait_recv()

    def gy_send(d, j):
        ref = out.at[:, wide(t, j)]
        return remote(ref, ref, GY, gy_r.at[seen(d), j], tp=tp_of(yo(d), c))

    def gy_recv(d, j):
        ref = out.at[:, wide(tp_of(yo(d), c), j)]
        return remote(ref, ref, GY, gy_r.at[d - 1, j], tp=tp_of(yo(d), c))

    def gc_send(d, j):
        ref = out.at[:, wide(tp_of(yo(d), c), j)]
        return remote(ref, ref, GC, gc_r.at[0], tp=tp_of(y, oc))

    pick0 = picker(slot0).astype(BF16)
    pick1 = picker(slot1).astype(BF16)
    rw0 = column(rw[0:1, :])
    rw1 = column(rw[1:2, :])
    for j in range(NF):
        mix0 = jnp.dot(pick0, ret[:, fold(j)], preferred_element_type=F32)
        mix1 = jnp.dot(pick1, ret[:, fold(j)], preferred_element_type=F32)
        out[:, wide(t, j)] = (
            mixed[:, fold(j)].astype(F32) + (rw0 * mix0 + rw1 * mix1)
        ).astype(BF16)
        for d in range(1, Y):
            gy_send(d, j).start()
        gc_send(0, j).start()

    @pl.when(me < S - 1)
    def _():
        remote(halo, halo, HALO, halo_r.at[0], sp=me + 1).wait_send()

    def drain(ref, sem):
        remote(ref, ref, sem, sem, tp=tp_of(y, oc)).wait_send()

    drain(rc1, C1)
    drain(sb1.at[pl.ds(0, Y - 1)], Y1)
    drain(ret.at[others], A)
    drain(x_all.at[:, pl.ds(0, (Y - 1) * W)], FY)
    drain(x_all.at[:, pl.ds(0, Y * W)], FC)
    drain(x_all.at[:, pl.ds(0, Y * W)], C2)
    drain(x_all.at[:, pl.ds(0, (Y - 1) * W)], Y2)
    drain(ret.at[others], B)

    for j in range(NF):
        for d in range(1, Y):
            gy_recv(d, j).wait_recv()
            gc_send(d, j).start()
    ours = out.at[:, pl.ds(0, Y * W)]
    remote(ours, ours, GC, gc_r.at[0], tp=tp_of(y, oc)).wait_recv()
    drain(ours, GC)
    drain(out.at[:, pl.ds(0, (Y - 1) * W)], GY)


def per_device(
    S,
    T,
    queries,
    key_rows,
    value_rows,
    sink_logits,
    out_weight,
    residual,
    norm_gain,
    routes,
    route_weights,
    gate_weight,
    up_weight,
    down_weight,
):
    R, D = residual.shape
    HW = queries.shape[1]
    Y = T // CORES
    W = D // T
    C = 2 * R * TOP // S
    FL = gate_weight.shape[2]
    NH = 4 if W % 512 == 0 else 1
    NF = 2 if W % 256 == 0 else 1
    hbm = pl.BlockSpec(memory_space=pl.ANY)
    dma = pltpu.SemaphoreType.DMA
    v = pltpu.VMEM
    return pl.pallas_call(
        functools.partial(kernel, S, T),
        out_shape=v((R, D), BF16),
        in_specs=[hbm] * 12,
        out_specs=pl.BlockSpec(memory_space=v),
        scratch_shapes=[
            v((1, sink_logits.shape[0]), F32),
            v(queries.shape, BF16),
            v(key_rows.shape, BF16),
            v(value_rows.shape, BF16),
            v((R, W), BF16),
            v((1, D), F32),
            v((TOP, R), jnp.int32),
            v((TOP, R), F32),
            v(out_weight.shape, BF16),
            v(gate_weight.shape[1:], BF16),
            v(up_weight.shape[1:], BF16),
            v(down_weight.shape[1:], BF16),
            v((2,) + key_rows.shape, BF16),
            v((R, HW), BF16),
            v((R, D), BF16),
            v((Y, R, W), BF16),
            v((Y, NH, R, W // NH), BF16),
            v((Y, NH, R, W // NH), BF16),
            v((R, W), BF16),
            v((S * C, W), BF16),
            v((S * C, D), BF16),
            v((S * C, D), BF16),
            v((S * C, FL), BF16),
            v((S * C, D), BF16),
            v((Y, S * C, W), BF16),
            v((Y - 1, S * C, W), BF16),
            v((Y - 1, S * C, W), BF16),
            v((S * C, W), BF16),
            v((S * C, W), BF16),
            dma((12,)),
            dma((11,)),
            dma((2,)),
            dma((Y,)),
            dma((Y - 1, NH)),
            dma((S, NF)),
            dma((S, Y - 1, NF)),
            dma((S,)),
            dma((3, Y)),
            dma((S, Y - 1, NF)),
            dma((1,)),
            dma((Y - 1, NF)),
            dma((1,)),
        ],
        compiler_params=pltpu.CompilerParams(
            collective_id=0, has_side_effects=True, vmem_limit_bytes=60 * 1024 * 1024
        ),
        name="layer",
    )(
        sink_logits.reshape(1, -1),
        queries,
        key_rows,
        value_rows,
        residual,
        norm_gain.reshape(1, D),
        routes.T,
        route_weights.T,
        out_weight,
        gate_weight,
        up_weight,
        down_weight,
    )


def solution(mesh):
    placed = (
        P("sp", "tp"),
        P("sp", "tp"),
        P("sp", "tp"),
        P("tp"),
        P("tp", None),
        P("sp", None),
        P(),
        P("sp", None),
        P("sp", None),
        P("sp", None, "tp"),
        P("sp", None, "tp"),
        P("sp", "tp", None),
    )
    return jax.shard_map(
        functools.partial(per_device, mesh.shape["sp"], mesh.shape["tp"]),
        mesh=mesh,
        in_specs=placed,
        out_specs=P("sp", None),
        check_vma=False,
    )
```

```python
import functools

import jax
import jax.numpy as jnp
import numpy as np
from jax import lax
from jax.experimental import pallas as pl
from jax.experimental.pallas import tpu as pltpu
from jax.sharding import PartitionSpec as P

HEAD_DIM = 64
WINDOW = 128
TOP = 2
CORES = 2
F32 = jnp.float32
BF16 = jnp.bfloat16
MESH = pl.DeviceIdType.MESH


def kernel(
    S,
    T,
    sink_hbm,
    q_hbm,
    k_hbm,
    v_hbm,
    res_hbm,
    gain_hbm,
    routes_hbm,
    rw_hbm,
    wo_hbm,
    wg_hbm,
    wu_hbm,
    wd_hbm,
    out,
    sink,
    q,
    k,
    v,
    res,
    gain,
    routes,
    rw,
    wo,
    wg,
    wu,
    wd,
    halo,
    att,
    pp,
    rc1,
    sb1,
    ry1,
    mixed,
    picked,
    x_all,
    xn,
    act,
    yp,
    rc2,
    sb2,
    ry2,
    rb,
    ret,
    w_sem,
    met,
    sent,
    halo_r,
    c1_r,
    y1_r,
    a_r,
    fy_r,
    fc_r,
    c2_r,
    y2_r,
    b_r,
    gy_r,
    gc_r,
):
    R, W = res.shape
    D = W * T
    Y = T // CORES
    H = q.shape[1] // HEAD_DIM
    KV = k.shape[1] // HEAD_DIM
    G = H // KV
    C = x_all.shape[0] // S
    Z = S // 2
    FL = wg.shape[1]
    NH = y1_r.shape[1]
    HALO, C1, Y1, A, FY, FC, C2, Y2, B, GY, GC = (sent.at[i] for i in range(11))
    HW = W // NH
    NF = gy_r.shape[1]
    FW = W // NF

    me = lax.axis_index("sp")
    t = lax.axis_index("tp")
    y = t // CORES
    c = t % CORES
    oc = 1 - c
    z = me // 2
    x = me % 2

    def tp_of(yy, cc):
        return yy * CORES + cc

    def cols(tt):
        return pl.ds(pl.multiple_of(tt * W, W), W)

    def part(tt, j):
        return pl.ds(pl.multiple_of(tt * W + j * HW, HW), HW)

    def wide(tt, f):
        return pl.ds(pl.multiple_of(tt * W + f * FW, FW), FW)

    def fold(f):
        return pl.ds(f * FW, FW)

    def rows(s):
        return pl.ds(pl.multiple_of(s * C, C), C)

    def yo(d):
        return (y + d) % Y

    def seen(d):
        return Y - d - 1

    def remote(src, dst, ss, rs, **dev):
        return pltpu.make_async_remote_copy(
            src_ref=src, dst_ref=dst, send_sem=ss, recv_sem=rs, device_id=dev, device_id_type=MESH
        )

    places = [(0, 0), (1, 0)] + [(0, d) for d in range(1, Z)] + [(1, d) for d in range(1, Z)]
    split = min(3, Z + 1)
    first = list(range(split))
    second = list(range(split, Z + 1))
    third = list(range(Z + 1, S))

    def peer(p):
        parity, bits = places[p]
        zz = z
        bit = 1
        while bit < Z:
            if bits // bit % 2:
                zz = zz + bit * (1 - 2 * (zz // bit % 2))
            bit *= 2
        return 2 * zz + (x + parity) % 2

    def span(p):
        return pl.ds(p * C, C)

    def block(group):
        return pl.ds(group[0] * C, len(group) * C)

    barrier = pltpu.get_barrier_semaphore()

    def greet(sem, step):
        for ok, e in ((me >= step, me - step), (me + step < S, me + step)):

            @pl.when(ok)
            def _(e=e):
                pl.semaphore_signal(sem, inc=1, device_id={"sp": e}, device_id_type=MESH)

    def greeted(sem, step, more=0):
        both = jnp.minimum(me // step, 1) + jnp.minimum((S - 1 - me) // step, 1)
        pl.semaphore_wait(sem, both + more)

    reach = [1]
    while 2 * reach[-1] < S:
        reach.append(2 * reach[-1])

    def meet(i):
        if i:
            greeted(met.at[i - 1], reach[i - 1])
        if i < len(reach):
            greet(met.at[i], reach[i])

    greet(barrier, 1)
    for d in range(1, Y):
        pl.semaphore_signal(
            barrier, inc=1, device_id={"tp": tp_of(yo(d), c)}, device_id_type=MESH
        )
    pl.semaphore_signal(barrier, inc=1, device_id={"tp": tp_of(y, oc)}, device_id_type=MESH)

    loads = [
        pltpu.make_async_copy(src, dst, w_sem.at[i])
        for i, (src, dst) in enumerate(
            (
                (k_hbm, k),
                (v_hbm, v),
                (q_hbm, q),
                (routes_hbm, routes),
                (sink_hbm, sink),
                (res_hbm.at[:, cols(t)], res),
                (rw_hbm, rw),
                (gain_hbm, gain),
                (wo_hbm, wo),
                (wg_hbm.at[0], wg),
                (wu_hbm.at[0], wu),
                (wd_hbm.at[0], wd),
            )
        )
    ]
    for load in loads:
        load.start()
    loads[0].wait()
    loads[1].wait()
    greeted(barrier, 1, Y)

    halo_copies = [
        remote(src, halo.at[i], HALO, halo_r.at[i], sp=jnp.minimum(me + 1, S - 1))
        for i, src in enumerate((k, v))
    ]

    @pl.when(me < S - 1)
    def _():
        for copy in halo_copies:
            copy.start()

    meet(0)
    for load in loads[2:5]:
        load.wait()

    qi = lax.broadcasted_iota(jnp.int32, (R, R), 0)
    kj = lax.broadcasted_iota(jnp.int32, (R, R), 1)
    dist_own = (qi - kj).astype(F32)
    dist_old = (qi - kj + WINDOW).astype(F32)
    nt = (((1,), (1,)), ((), ()))

    ok_own = qi >= kj
    ok_old = (kj >= qi) & (kj + me * R >= WINDOW)

    base = jnp.float32(1.0)
    for i in range(1, T):
        base = jnp.where(t == i, jnp.float32(2.0 ** (-8.0 * i / T)), base)

    def head(h):
        return slice(h * HEAD_DIM, (h + 1) * HEAD_DIM), slice(
            (h // G) * HEAD_DIM, (h // G + 1) * HEAD_DIM
        )

    def scores(h, keys, dist, ok):
        raw = lax.dot_general(q[:, head(h)[0]], keys, nt, preferred_element_type=F32)
        slope = base * np.float32(2.0 ** (-8.0 * (h + 1) / (H * T)))
        return jnp.where(ok, raw * HEAD_DIM**-0.5 - slope * dist, -jnp.inf)

    s_own = [scores(h, k[:, head(h)[1]], dist_own, ok_own) for h in range(H)]
    top = [jnp.max(a, axis=1, keepdims=True) for a in s_own]
    e_own = [jnp.exp(a - b) for a, b in zip(s_own, top)]
    weight = [jnp.sum(a, axis=1, keepdims=True) for a in e_own]
    mix_own = [
        jnp.dot(a.astype(BF16), v[:, head(h)[1]], preferred_element_type=F32)
        for h, a in enumerate(e_own)
    ]

    meet(1)

    def column(row):
        return jnp.broadcast_to(row, (R, R)).T[:, 0:1]

    r0 = column(routes[0:1, :].astype(F32)).astype(jnp.int32)
    r1 = column(routes[1:2, :].astype(F32)).astype(jnp.int32)
    lane_e = lax.broadcasted_iota(jnp.int32, (R, 128), 1)
    hit0 = lane_e == r0
    hit1 = lane_e == r1
    member = jnp.where(hit0 | hit1, 1.0, 0.0).astype(BF16)
    tri = jnp.where(
        lax.broadcasted_iota(jnp.int32, (R, R), 1) < lax.broadcasted_iota(jnp.int32, (R, R), 0),
        1.0,
        0.0,
    ).astype(BF16)
    rank = jnp.dot(tri, member, preferred_element_type=F32)
    rank0 = jnp.sum(jnp.where(hit0, rank, 0.0), axis=1, keepdims=True)
    rank1 = jnp.sum(jnp.where(hit1, rank, 0.0), axis=1, keepdims=True)
    slot0 = r0.astype(F32) * C + rank0
    slot1 = r1.astype(F32) * C + rank1
    lane_s = lax.broadcasted_iota(jnp.int32, (R, S * C), 1).astype(F32)

    def picker(slot):
        return jnp.where(lane_s == slot, 1.0, 0.0)

    both = (picker(slot0) + picker(slot1)).T.astype(BF16)

    @pl.when(me > 0)
    def _():
        halo_copies[0].wait_recv()

    @pl.when(me == 0)
    def _():
        halo[...] = jnp.zeros_like(halo)

    s_old = [scores(h, halo[0, :, head(h)[1]], dist_old, ok_old) for h in range(H)]
    peak = [jnp.maximum(a, jnp.max(b, axis=1, keepdims=True)) for a, b in zip(top, s_old)]
    shrink = [jnp.exp(a - b) for a, b in zip(top, peak)]
    e_old = [jnp.exp(a - b) for a, b in zip(s_old, peak)]
    total = [
        a * b + jnp.sum(e, axis=1, keepdims=True) for a, b, e in zip(weight, shrink, e_old)
    ]
    keep = [
        1.0 / (a + jnp.exp(sink[0:1, h : h + 1] - b)) for h, (a, b) in enumerate(zip(total, peak))
    ]

    @pl.when(me > 0)
    def _():
        halo_copies[1].wait_recv()

    mix_old = [
        jnp.dot(a.astype(BF16), halo[1, :, head(h)[1]], preferred_element_type=F32)
        for h, a in enumerate(e_old)
    ]
    for h in range(H):
        att[:, head(h)[0]] = ((mix_own[h] * shrink[h] + mix_old[h]) * keep[h]).astype(BF16)

    meet(2)
    for load in loads[5:9]:
        load.wait()

    def project(tt):
        pp[:, cols(tt)] = jnp.dot(att[...], wo[:, cols(tt)], preferred_element_type=F32).astype(
            BF16
        )

    def c1(yy):
        return remote(
            pp.at[:, cols(tp_of(yy, oc))], rc1.at[yy], C1, c1_r.at[yy], tp=tp_of(y, oc)
        )

    def y1_send(d, j):
        yy = yo(d)
        return remote(
            sb1.at[yy, j], ry1.at[y, j], Y1, y1_r.at[seen(d), j], tp=tp_of(yy, c)
        )

    def y1_recv(d, j):
        yy = yo(d)
        return remote(sb1.at[yy, j], ry1.at[yy, j], Y1, y1_r.at[d - 1, j], tp=tp_of(yy, c))

    turns = list(range(1, Y)) + [0]

    def half(j):
        return slice(j * HW, (j + 1) * HW)

    for d in turns[:-1]:
        project(tp_of(yo(d), oc))
        c1(yo(d)).start()
    for d in turns[:-1]:
        project(tp_of(yo(d), c))
    for d in turns[:-1]:
        c1(yo(d)).wait_recv()
        for j in range(NH):
            sb1[yo(d), j] = (
                pp[:, part(tp_of(yo(d), c), j)].astype(F32) + rc1[yo(d), :, half(j)].astype(F32)
            ).astype(BF16)
            y1_send(d, j).start()
    project(tp_of(y, oc))
    c1(y).start()
    project(t)
    c1(y).wait_recv()
    for i in range(3, len(reach) + 1):
        meet(i)

    def a_send(p, j):
        e = peer(p)
        return remote(
            picked.at[rows(e), half(j)],
            x_all.at[span(p), part(t, j)],
            A,
            a_r.at[p, j * NF // NH],
            sp=e,
        )

    def a_fold(p, f):
        e = peer(p)
        return remote(
            picked.at[rows(e), fold(f)], x_all.at[span(p), wide(t, f)], A, a_r.at[p, f], sp=e
        )

    def fy_send(p, d, f):
        ref = x_all.at[span(p), wide(t, f)]
        return remote(ref, ref, FY, fy_r.at[p, seen(d), f], tp=tp_of(yo(d), c))

    def fy_recv(p, d, f):
        ref = x_all.at[span(p), wide(tp_of(yo(d), c), f)]
        return remote(ref, ref, FY, fy_r.at[p, d - 1, f], tp=tp_of(yo(d), c))

    def fc_send(p, d, f):
        ref = x_all.at[span(p), wide(tp_of(yo(d), c), f)]
        return remote(ref, ref, FC, fc_r.at[p], tp=tp_of(y, oc))

    def fc_recv(p):
        ref = x_all.at[span(p), pl.ds(0, Y * W)]
        return remote(ref, ref, FC, fc_r.at[p], tp=tp_of(y, oc))

    arrivals = list(range(1, Z + 1))

    for j in range(NH):
        head_sum = pp[:, part(t, j)].astype(F32) + rc1[y, :, half(j)].astype(F32)
        for d in range(1, Y):
            y1_recv(d, j).wait_recv()
            head_sum = head_sum + ry1[yo(d), j].astype(F32)
        mixed[:, half(j)] = (res[:, half(j)].astype(F32) + head_sum).astype(BF16)
        picked[:, half(j)] = jnp.dot(
            both, mixed[:, half(j)], preferred_element_type=F32
        ).astype(BF16)
        for p in arrivals:
            a_send(p, j).start()
    x_all[span(0), cols(t)] = picked[rows(me)]

    def forward(p, f):
        for d in range(1, Y):
            fy_send(p, d, f).start()
        fc_send(p, 0, f).start()

    def relay(p):
        for f in range(NF):
            for d in range(1, Y):
                fy_recv(p, d, f).wait_recv()
                fc_send(p, d, f).start()

    def arrive(p):
        for f in range(NF):
            a_fold(p, f).wait_recv()
            forward(p, f)

    def norm(p):
        fc_recv(p).wait_recv()
        wide = x_all[span(p)].astype(F32)
        scale = lax.rsqrt(jnp.mean(wide * wide, axis=1, keepdims=True) + 1e-06)
        xn[span(p)] = (wide * scale * gain[...]).astype(BF16)

    TN = min(256, FL)
    NT = FL // TN

    def hidden(group, hooks):
        at = block(group)

        @pl.loop(0, NT)
        def _(n):
            nn = pl.ds(pl.multiple_of(n * TN, TN), TN)
            gate = jnp.dot(xn[at], wg[:, nn], preferred_element_type=F32)
            up = jnp.dot(xn[at], wu[:, nn], preferred_element_type=F32)
            act[at, nn] = (gate / (1.0 + jnp.exp(-gate)) * up).astype(BF16)
            for i in range(NT):
                todo = [hook for turn, hook in hooks if min(turn, NT - 1) == i]
                if todo:

                    @pl.when(n == i)
                    def _(todo=todo):
                        for hook in todo:
                            hook()

    def c2(g, d):
        at = block(groups[g])
        return remote(
            yp.at[at, cols(tp_of(yo(d), oc))], rc2.at[d, at], C2, c2_r.at[g, d], tp=tp_of(y, oc)
        )

    def down_block(g, tt):
        at = block(groups[g])
        yp[at, cols(tt)] = jnp.dot(act[at], wd[:, cols(tt)], preferred_element_type=F32).astype(
            BF16
        )

    def y2_send(p, d, f):
        return remote(
            sb2.at[d - 1, span(p), fold(f)],
            ry2.at[seen(d), span(p), fold(f)],
            Y2,
            y2_r.at[p, seen(d), f],
            tp=tp_of(yo(d), c),
        )

    def y2_recv(p, d, f):
        return remote(
            sb2.at[d - 1, span(p), fold(f)],
            ry2.at[d - 1, span(p), fold(f)],
            Y2,
            y2_r.at[p, d - 1, f],
            tp=tp_of(yo(d), c),
        )

    groups = [g for g in (first, second, third) if g]
    back = [g[:0:-1] + g[:1] if g is first else g[1:] + g[:1] for g in groups]

    def pair_sum(g, d):
        c2(g, d).wait_recv()
        for p in back[g]:
            at = span(p)
            sb2[d - 1, at] = (
                yp[at, cols(tp_of(yo(d), c))].astype(F32) + rc2[d, at].astype(F32)
            ).astype(BF16)
            for f in range(NF):
                y2_send(p, d, f).start()

    def down(g, turn):
        for d in turn:
            down_block(g, tp_of(yo(d), oc))
            c2(g, d).start()
        for d in turn:
            down_block(g, tp_of(yo(d), c))

    def b_send(p, f):
        e = peer(p)
        return remote(
            rb.at[span(p), fold(f)], ret.at[rows(me), fold(f)], B, b_r.at[0], sp=e
        )

    def send_back(p):
        at = span(p)
        for f in range(NF):
            total = yp[at, wide(t, f)].astype(F32) + rc2[0, at, fold(f)].astype(F32)
            for d in range(1, Y):
                y2_recv(p, d, f).wait_recv()
                total = total + ry2[d - 1, at, fold(f)].astype(F32)
            if p:
                rb[at, fold(f)] = total.astype(BF16)
                b_send(p, f).start()
            else:
                ret[rows(me), fold(f)] = total.astype(BF16)

    def later(f, *args):
        return lambda: f(*args)

    for f in range(NF):
        forward(0, f)
    for i, p in enumerate(arrivals):
        arrive(p)
        if i == 0:
            for q in third:
                for f in range(NF):
                    a_fold(q, f).start()
        elif p <= split:
            relay(p - 2)
    for p in range(min(split, Z) - 1, split):
        relay(p)
    for p in first:
        norm(p)
    loads[9].wait()
    loads[10].wait()
    steps = [later(arrive, p) for p in third[:1]] + [later(relay, p) for p in second]
    steps += [later(arrive, p) for p in third[1:2]]
    hidden(first, [(i, step) for i, step in enumerate(steps)])
    loads[11].wait()
    last = len(groups) - 1
    if second:
        for p in second:
            norm(p)
        steps = [later(arrive, p) for p in third[2:]] + [later(relay, p) for p in third[:-2]]
        hidden(second, [(i, step) for i, step in enumerate(steps)])
        down(1, turns[:-1])
    else:
        for p in third[2:]:
            arrive(p)
        for p in third[:-2]:
            relay(p)
    down(0, turns[:-1])
    relay(third[-2])
    if second:
        for d in turns[:-1]:
            pair_sum(1, d)
        down(1, turns[-1:])
    for d in turns[:-1]:
        pair_sum(0, d)
    relay(third[-1])
    for p in third[:-1]:
        norm(p)
    down(0, turns[-1:])
    for g in range(last):
        c2(g, 0).wait_recv()
    norm(third[-1])
    steps = [later(send_back, p) for p in back[1]] if second else []
    hidden(third, [(2 * i + 1, step) for i, step in enumerate(steps)])
    down(last, turns[:-1])
    down_block(last, tp_of(y, oc))
    c2(last, 0).start()
    for d in turns[:-1]:
        pair_sum(last, d)
    down_block(last, t)
    c2(last, 0).wait_recv()
    for p in back[0] + back[-1]:
        send_back(p)

    others = pl.ds(0, (S - 1) * C)
    remote(rb.at[others], ret.at[others], B, b_r.at[0], sp=peer(1)).wait_recv()

    def gy_send(d, j):
        ref = out.at[:, wide(t, j)]
        return remote(ref, ref, GY, gy_r.at[seen(d), j], tp=tp_of(yo(d), c))

    def gy_recv(d, j):
        ref = out.at[:, wide(tp_of(yo(d), c), j)]
        return remote(ref, ref, GY, gy_r.at[d - 1, j], tp=tp_of(yo(d), c))

    def gc_send(d, j):
        ref = out.at[:, wide(tp_of(yo(d), c), j)]
        return remote(ref, ref, GC, gc_r.at[0], tp=tp_of(y, oc))

    pick0 = picker(slot0).astype(BF16)
    pick1 = picker(slot1).astype(BF16)
    rw0 = column(rw[0:1, :])
    rw1 = column(rw[1:2, :])
    for j in range(NF):
        mix0 = jnp.dot(pick0, ret[:, fold(j)], preferred_element_type=F32)
        mix1 = jnp.dot(pick1, ret[:, fold(j)], preferred_element_type=F32)
        out[:, wide(t, j)] = (
            mixed[:, fold(j)].astype(F32) + (rw0 * mix0 + rw1 * mix1)
        ).astype(BF16)
        for d in range(1, Y):
            gy_send(d, j).start()
        gc_send(0, j).start()

    @pl.when(me < S - 1)
    def _():
        remote(halo, halo, HALO, halo_r.at[0], sp=me + 1).wait_send()

    def drain(ref, sem):
        remote(ref, ref, sem, sem, tp=tp_of(y, oc)).wait_send()

    drain(rc1, C1)
    drain(sb1.at[pl.ds(0, Y - 1)], Y1)
    drain(ret.at[others], A)
    drain(x_all.at[:, pl.ds(0, (Y - 1) * W)], FY)
    drain(x_all.at[:, pl.ds(0, Y * W)], FC)
    drain(x_all.at[:, pl.ds(0, Y * W)], C2)
    drain(x_all.at[:, pl.ds(0, (Y - 1) * W)], Y2)
    drain(ret.at[others], B)

    for j in range(NF):
        for d in range(1, Y):
            gy_recv(d, j).wait_recv()
            gc_send(d, j).start()
    ours = out.at[:, pl.ds(0, Y * W)]
    remote(ours, ours, GC, gc_r.at[0], tp=tp_of(y, oc)).wait_recv()
    drain(ours, GC)
    drain(out.at[:, pl.ds(0, (Y - 1) * W)], GY)


def per_device(
    S,
    T,
    queries,
    key_rows,
    value_rows,
    sink_logits,
    out_weight,
    residual,
    norm_gain,
    routes,
    route_weights,
    gate_weight,
    up_weight,
    down_weight,
):
    R, D = residual.shape
    HW = queries.shape[1]
    Y = T // CORES
    W = D // T
    C = 2 * R * TOP // S
    FL = gate_weight.shape[2]
    NH = 4 if W % 512 == 0 else 1
    NF = 2 if W % 256 == 0 else 1
    hbm = pl.BlockSpec(memory_space=pl.ANY)
    dma = pltpu.SemaphoreType.DMA
    v = pltpu.VMEM
    return pl.pallas_call(
        functools.partial(kernel, S, T),
        out_shape=v((R, D), BF16),
        in_specs=[hbm] * 12,
        out_specs=pl.BlockSpec(memory_space=v),
        scratch_shapes=[
            v((1, sink_logits.shape[0]), F32),
            v(queries.shape, BF16),
            v(key_rows.shape, BF16),
            v(value_rows.shape, BF16),
            v((R, W), BF16),
            v((1, D), F32),
            v((TOP, R), jnp.int32),
            v((TOP, R), F32),
            v(out_weight.shape, BF16),
            v(gate_weight.shape[1:], BF16),
            v(up_weight.shape[1:], BF16),
            v(down_weight.shape[1:], BF16),
            v((2,) + key_rows.shape, BF16),
            v((R, HW), BF16),
            v((R, D), BF16),
            v((Y, R, W), BF16),
            v((Y, NH, R, W // NH), BF16),
            v((Y, NH, R, W // NH), BF16),
            v((R, W), BF16),
            v((S * C, W), BF16),
            v((S * C, D), BF16),
            v((S * C, D), BF16),
            v((S * C, FL), BF16),
            v((S * C, D), BF16),
            v((Y, S * C, W), BF16),
            v((Y - 1, S * C, W), BF16),
            v((Y - 1, S * C, W), BF16),
            v((S * C, W), BF16),
            v((S * C, W), BF16),
            dma((12,)),
            pltpu.SemaphoreType.REGULAR((max(1, (S - 1).bit_length()),)),
            dma((11,)),
            dma((2,)),
            dma((Y,)),
            dma((Y - 1, NH)),
            dma((S, NF)),
            dma((S, Y - 1, NF)),
            dma((S,)),
            dma((3, Y)),
            dma((S, Y - 1, NF)),
            dma((1,)),
            dma((Y - 1, NF)),
            dma((1,)),
        ],
        compiler_params=pltpu.CompilerParams(
            collective_id=0, has_side_effects=True, vmem_limit_bytes=60 * 1024 * 1024
        ),
        name="layer",
    )(
        sink_logits.reshape(1, -1),
        queries,
        key_rows,
        value_rows,
        residual,
        norm_gain.reshape(1, D),
        routes.T,
        route_weights.T,
        out_weight,
        gate_weight,
        up_weight,
        down_weight,
    )


def solution(mesh):
    placed = (
        P("sp", "tp"),
        P("sp", "tp"),
        P("sp", "tp"),
        P("tp"),
        P("tp", None),
        P("sp", None),
        P(),
        P("sp", None),
        P("sp", None),
        P("sp", None, "tp"),
        P("sp", None, "tp"),
        P("sp", "tp", None),
    )
    return jax.shard_map(
        functools.partial(per_device, mesh.shape["sp"], mesh.shape["tp"]),
        mesh=mesh,
        in_specs=placed,
        out_specs=P("sp", None),
        check_vma=False,
    )
```

```python
import functools

import jax
import jax.numpy as jnp
import numpy as np
from jax import lax
from jax.experimental import pallas as pl
from jax.experimental.pallas import tpu as pltpu
from jax.sharding import PartitionSpec as P

HEAD_DIM = 64
WINDOW = 128
TOP = 2
CORES = 2
F32 = jnp.float32
BF16 = jnp.bfloat16
MESH = pl.DeviceIdType.MESH


def kernel(
    S,
    T,
    sink_hbm,
    q_hbm,
    k_hbm,
    v_hbm,
    res_hbm,
    gain_hbm,
    routes_hbm,
    rw_hbm,
    wo_hbm,
    wg_hbm,
    wu_hbm,
    wd_hbm,
    out,
    sink,
    q,
    k,
    v,
    res,
    gain,
    routes,
    rw,
    wo,
    wg,
    wu,
    wd,
    halo,
    att,
    pp,
    rc1,
    sb1,
    ry1,
    mixed,
    picked,
    x_all,
    xn,
    act,
    yp,
    rc2,
    sb2,
    ry2,
    rb,
    ret,
    w_sem,
    met,
    sent,
    halo_r,
    c1_r,
    y1_r,
    a_r,
    fy_r,
    fc_r,
    c2_r,
    y2_r,
    b_r,
    gy_r,
    gc_r,
):
    R, W = res.shape
    D = W * T
    Y = T // CORES
    H = q.shape[1] // HEAD_DIM
    KV = k.shape[1] // HEAD_DIM
    G = H // KV
    C = x_all.shape[0] // S
    Z = S // 2
    FL = wg.shape[1]
    NH = y1_r.shape[1]
    HALO, C1, Y1, A, FY, FC, C2, Y2, B, GY, GC = (sent.at[i] for i in range(11))
    HW = W // NH
    NF = a_r.shape[1]
    NG = gy_r.shape[1]
    GW = W // NG
    FW = W // NF

    me = lax.axis_index("sp")
    t = lax.axis_index("tp")
    y = t // CORES
    c = t % CORES
    oc = 1 - c
    z = me // 2
    x = me % 2

    def tp_of(yy, cc):
        return yy * CORES + cc

    def cols(tt):
        return pl.ds(pl.multiple_of(tt * W, W), W)

    def part(tt, j):
        return pl.ds(pl.multiple_of(tt * W + j * HW, HW), HW)

    def wide(tt, f):
        return pl.ds(pl.multiple_of(tt * W + f * FW, FW), FW)

    def fold(f):
        return pl.ds(f * FW, FW)

    def rows(s):
        return pl.ds(pl.multiple_of(s * C, C), C)

    def yo(d):
        return (y + d) % Y

    def seen(d):
        return Y - d - 1

    def remote(src, dst, ss, rs, **dev):
        return pltpu.make_async_remote_copy(
            src_ref=src, dst_ref=dst, send_sem=ss, recv_sem=rs, device_id=dev, device_id_type=MESH
        )

    places = [(0, 0), (1, 0)] + [(0, d) for d in range(1, Z)] + [(1, d) for d in range(1, Z)]
    split = min(3, Z + 1)
    first = list(range(split))
    second = list(range(split, Z + 1))
    third = list(range(Z + 1, S))

    def peer(p):
        parity, bits = places[p]
        zz = z
        bit = 1
        while bit < Z:
            if bits // bit % 2:
                zz = zz + bit * (1 - 2 * (zz // bit % 2))
            bit *= 2
        return 2 * zz + (x + parity) % 2

    def span(p):
        return pl.ds(p * C, C)

    def block(group):
        return pl.ds(group[0] * C, len(group) * C)

    barrier = pltpu.get_barrier_semaphore()

    def greet(sem, step):
        for ok, e in ((me >= step, me - step), (me + step < S, me + step)):

            @pl.when(ok)
            def _(e=e):
                pl.semaphore_signal(sem, inc=1, device_id={"sp": e}, device_id_type=MESH)

    def greeted(sem, step, more=0):
        both = jnp.minimum(me // step, 1) + jnp.minimum((S - 1 - me) // step, 1)
        pl.semaphore_wait(sem, both + more)

    reach = [1]
    while 2 * reach[-1] < S:
        reach.append(2 * reach[-1])

    def meet(i):
        if i:
            greeted(met.at[i - 1], reach[i - 1])
        if i < len(reach):
            greet(met.at[i], reach[i])

    greet(barrier, 1)
    for d in range(1, Y):
        pl.semaphore_signal(
            barrier, inc=1, device_id={"tp": tp_of(yo(d), c)}, device_id_type=MESH
        )
    pl.semaphore_signal(barrier, inc=1, device_id={"tp": tp_of(y, oc)}, device_id_type=MESH)

    loads = [
        pltpu.make_async_copy(src, dst, w_sem.at[i])
        for i, (src, dst) in enumerate(
            (
                (k_hbm, k),
                (v_hbm, v),
                (q_hbm, q),
                (routes_hbm, routes),
                (sink_hbm, sink),
                (res_hbm.at[:, cols(t)], res),
                (rw_hbm, rw),
                (gain_hbm, gain),
                (wo_hbm, wo),
                (wg_hbm.at[0], wg),
                (wu_hbm.at[0], wu),
                (wd_hbm.at[0], wd),
            )
        )
    ]
    for load in loads:
        load.start()
    loads[0].wait()
    loads[1].wait()
    greeted(barrier, 1, Y)

    halo_copies = [
        remote(src, halo.at[i], HALO, halo_r.at[i], sp=jnp.minimum(me + 1, S - 1))
        for i, src in enumerate((k, v))
    ]

    @pl.when(me < S - 1)
    def _():
        for copy in halo_copies:
            copy.start()

    meet(0)
    for load in loads[2:5]:
        load.wait()

    qi = lax.broadcasted_iota(jnp.int32, (R, R), 0)
    kj = lax.broadcasted_iota(jnp.int32, (R, R), 1)
    dist_own = (qi - kj).astype(F32)
    dist_old = (qi - kj + WINDOW).astype(F32)
    nt = (((1,), (1,)), ((), ()))

    ok_own = qi >= kj
    ok_old = (kj >= qi) & (kj + me * R >= WINDOW)

    base = jnp.float32(1.0)
    for i in range(1, T):
        base = jnp.where(t == i, jnp.float32(2.0 ** (-8.0 * i / T)), base)

    def head(h):
        return slice(h * HEAD_DIM, (h + 1) * HEAD_DIM), slice(
            (h // G) * HEAD_DIM, (h // G + 1) * HEAD_DIM
        )

    def scores(h, keys, dist, ok):
        raw = lax.dot_general(q[:, head(h)[0]], keys, nt, preferred_element_type=F32)
        slope = base * np.float32(2.0 ** (-8.0 * (h + 1) / (H * T)))
        return jnp.where(ok, raw * HEAD_DIM**-0.5 - slope * dist, -jnp.inf)

    s_own = [scores(h, k[:, head(h)[1]], dist_own, ok_own) for h in range(H)]
    top = [jnp.max(a, axis=1, keepdims=True) for a in s_own]
    e_own = [jnp.exp(a - b) for a, b in zip(s_own, top)]
    weight = [jnp.sum(a, axis=1, keepdims=True) for a in e_own]
    mix_own = [
        jnp.dot(a.astype(BF16), v[:, head(h)[1]], preferred_element_type=F32)
        for h, a in enumerate(e_own)
    ]

    meet(1)

    def column(row):
        return jnp.broadcast_to(row, (R, R)).T[:, 0:1]

    r0 = column(routes[0:1, :].astype(F32)).astype(jnp.int32)
    r1 = column(routes[1:2, :].astype(F32)).astype(jnp.int32)
    lane_e = lax.broadcasted_iota(jnp.int32, (R, 128), 1)
    hit0 = lane_e == r0
    hit1 = lane_e == r1
    member = jnp.where(hit0 | hit1, 1.0, 0.0).astype(BF16)
    tri = jnp.where(
        lax.broadcasted_iota(jnp.int32, (R, R), 1) < lax.broadcasted_iota(jnp.int32, (R, R), 0),
        1.0,
        0.0,
    ).astype(BF16)
    rank = jnp.dot(tri, member, preferred_element_type=F32)
    rank0 = jnp.sum(jnp.where(hit0, rank, 0.0), axis=1, keepdims=True)
    rank1 = jnp.sum(jnp.where(hit1, rank, 0.0), axis=1, keepdims=True)
    slot0 = r0.astype(F32) * C + rank0
    slot1 = r1.astype(F32) * C + rank1
    lane_s = lax.broadcasted_iota(jnp.int32, (R, S * C), 1).astype(F32)

    def picker(slot):
        return jnp.where(lane_s == slot, 1.0, 0.0)

    both = (picker(slot0) + picker(slot1)).T.astype(BF16)

    @pl.when(me > 0)
    def _():
        halo_copies[0].wait_recv()

    @pl.when(me == 0)
    def _():
        halo[...] = jnp.zeros_like(halo)

    s_old = [scores(h, halo[0, :, head(h)[1]], dist_old, ok_old) for h in range(H)]
    peak = [jnp.maximum(a, jnp.max(b, axis=1, keepdims=True)) for a, b in zip(top, s_old)]
    shrink = [jnp.exp(a - b) for a, b in zip(top, peak)]
    e_old = [jnp.exp(a - b) for a, b in zip(s_old, peak)]
    total = [
        a * b + jnp.sum(e, axis=1, keepdims=True) for a, b, e in zip(weight, shrink, e_old)
    ]
    keep = [
        1.0 / (a + jnp.exp(sink[0:1, h : h + 1] - b)) for h, (a, b) in enumerate(zip(total, peak))
    ]

    @pl.when(me > 0)
    def _():
        halo_copies[1].wait_recv()

    mix_old = [
        jnp.dot(a.astype(BF16), halo[1, :, head(h)[1]], preferred_element_type=F32)
        for h, a in enumerate(e_old)
    ]
    for h in range(H):
        att[:, head(h)[0]] = ((mix_own[h] * shrink[h] + mix_old[h]) * keep[h]).astype(BF16)

    meet(2)
    for load in loads[5:9]:
        load.wait()

    def project(tt):
        pp[:, cols(tt)] = jnp.dot(att[...], wo[:, cols(tt)], preferred_element_type=F32).astype(
            BF16
        )

    def c1(yy):
        return remote(
            pp.at[:, cols(tp_of(yy, oc))], rc1.at[yy], C1, c1_r.at[yy], tp=tp_of(y, oc)
        )

    def y1_send(d, j):
        yy = yo(d)
        return remote(
            sb1.at[yy, j], ry1.at[y, j], Y1, y1_r.at[seen(d), j], tp=tp_of(yy, c)
        )

    def y1_recv(d, j):
        yy = yo(d)
        return remote(sb1.at[yy, j], ry1.at[yy, j], Y1, y1_r.at[d - 1, j], tp=tp_of(yy, c))

    turns = list(range(1, Y)) + [0]

    def half(j):
        return slice(j * HW, (j + 1) * HW)

    for d in turns[:-1]:
        project(tp_of(yo(d), oc))
        c1(yo(d)).start()
    for d in turns[:-1]:
        project(tp_of(yo(d), c))
    for d in turns[:-1]:
        c1(yo(d)).wait_recv()
        for j in range(NH):
            sb1[yo(d), j] = (
                pp[:, part(tp_of(yo(d), c), j)].astype(F32) + rc1[yo(d), :, half(j)].astype(F32)
            ).astype(BF16)
            y1_send(d, j).start()
    project(tp_of(y, oc))
    c1(y).start()
    project(t)
    c1(y).wait_recv()
    for i in range(3, len(reach) + 1):
        meet(i)

    def a_send(p, j):
        e = peer(p)
        return remote(
            picked.at[rows(e), half(j)],
            x_all.at[span(p), part(t, j)],
            A,
            a_r.at[p, j * NF // NH],
            sp=e,
        )

    def a_fold(p, f):
        e = peer(p)
        return remote(
            picked.at[rows(e), fold(f)], x_all.at[span(p), wide(t, f)], A, a_r.at[p, f], sp=e
        )

    def fy_send(p, d, f):
        ref = x_all.at[span(p), wide(t, f)]
        return remote(ref, ref, FY, fy_r.at[p, seen(d), f], tp=tp_of(yo(d), c))

    def fy_recv(p, d, f):
        ref = x_all.at[span(p), wide(tp_of(yo(d), c), f)]
        return remote(ref, ref, FY, fy_r.at[p, d - 1, f], tp=tp_of(yo(d), c))

    def fc_send(p, d, f):
        ref = x_all.at[span(p), wide(tp_of(yo(d), c), f)]
        return remote(ref, ref, FC, fc_r.at[p], tp=tp_of(y, oc))

    def fc_recv(p):
        ref = x_all.at[span(p), pl.ds(0, Y * W)]
        return remote(ref, ref, FC, fc_r.at[p], tp=tp_of(y, oc))

    arrivals = list(range(1, Z + 1))

    for j in range(NH):
        head_sum = pp[:, part(t, j)].astype(F32) + rc1[y, :, half(j)].astype(F32)
        for d in range(1, Y):
            y1_recv(d, j).wait_recv()
            head_sum = head_sum + ry1[yo(d), j].astype(F32)
        mixed[:, half(j)] = (res[:, half(j)].astype(F32) + head_sum).astype(BF16)
        picked[:, half(j)] = jnp.dot(
            both, mixed[:, half(j)], preferred_element_type=F32
        ).astype(BF16)
        for p in arrivals:
            a_send(p, j).start()
    for f in range(NF):
        a_fold(third[0], f).start()
    x_all[span(0), cols(t)] = picked[rows(me)]

    def forward(p, f):
        for d in range(1, Y):
            fy_send(p, d, f).start()
        fc_send(p, 0, f).start()

    def relay(p):
        for f in range(NF):
            for d in range(1, Y):
                fy_recv(p, d, f).wait_recv()
                fc_send(p, d, f).start()

    def arrive(p):
        for f in range(NF):
            a_fold(p, f).wait_recv()
            forward(p, f)

    def norm(p):
        fc_recv(p).wait_recv()
        wide = x_all[span(p)].astype(F32)
        scale = lax.rsqrt(jnp.mean(wide * wide, axis=1, keepdims=True) + 1e-06)
        xn[span(p)] = (wide * scale * gain[...]).astype(BF16)

    TN = min(256, FL)
    NT = FL // TN

    def hidden(group, hooks):
        at = block(group)

        @pl.loop(0, NT)
        def _(n):
            nn = pl.ds(pl.multiple_of(n * TN, TN), TN)
            gate = jnp.dot(xn[at], wg[:, nn], preferred_element_type=F32)
            up = jnp.dot(xn[at], wu[:, nn], preferred_element_type=F32)
            act[at, nn] = (gate / (1.0 + jnp.exp(-gate)) * up).astype(BF16)
            for i in range(NT):
                todo = [hook for turn, hook in hooks if min(turn, NT - 1) == i]
                if todo:

                    @pl.when(n == i)
                    def _(todo=todo):
                        for hook in todo:
                            hook()

    def c2(g, d):
        at = block(groups[g])
        return remote(
            yp.at[at, cols(tp_of(yo(d), oc))], rc2.at[d, at], C2, c2_r.at[g, d], tp=tp_of(y, oc)
        )

    def down_block(g, tt):
        at = block(groups[g])
        yp[at, cols(tt)] = jnp.dot(act[at], wd[:, cols(tt)], preferred_element_type=F32).astype(
            BF16
        )

    def y2_send(p, d, f):
        return remote(
            sb2.at[d - 1, span(p), fold(f)],
            ry2.at[seen(d), span(p), fold(f)],
            Y2,
            y2_r.at[p, seen(d), f],
            tp=tp_of(yo(d), c),
        )

    def y2_recv(p, d, f):
        return remote(
            sb2.at[d - 1, span(p), fold(f)],
            ry2.at[d - 1, span(p), fold(f)],
            Y2,
            y2_r.at[p, d - 1, f],
            tp=tp_of(yo(d), c),
        )

    groups = [g for g in (first, second, third) if g]
    back = [g[:0:-1] + g[:1] if g is first else g[1:] + g[:1] for g in groups]

    def pair_sum(g, d):
        c2(g, d).wait_recv()
        for p in back[g]:
            at = span(p)
            sb2[d - 1, at] = (
                yp[at, cols(tp_of(yo(d), c))].astype(F32) + rc2[d, at].astype(F32)
            ).astype(BF16)
            if p:
                for f in range(NF):
                    y2_send(p, d, f).start()

    def y2_own(d):
        for f in range(NF):
            y2_send(0, d, f).start()

    def down(g, turn):
        for d in turn:
            down_block(g, tp_of(yo(d), oc))
            c2(g, d).start()
        for d in turn:
            down_block(g, tp_of(yo(d), c))

    def b_send(p, f):
        e = peer(p)
        return remote(
            rb.at[span(p), fold(f)], ret.at[rows(me), fold(f)], B, b_r.at[0], sp=e
        )

    def send_back(p):
        at = span(p)
        for f in range(NF):
            total = yp[at, wide(t, f)].astype(F32) + rc2[0, at, fold(f)].astype(F32)
            for d in range(1, Y):
                y2_recv(p, d, f).wait_recv()
                total = total + ry2[d - 1, at, fold(f)].astype(F32)
            if p:
                rb[at, fold(f)] = total.astype(BF16)
                b_send(p, f).start()
            else:
                ret[rows(me), fold(f)] = total.astype(BF16)

    def later(f, *args):
        return lambda: f(*args)

    for f in range(NF):
        forward(0, f)
    for i, p in enumerate(arrivals):
        arrive(p)
        if i == 1:
            for q in third[1:]:
                for f in range(NF):
                    a_fold(q, f).start()
        if 1 <= i and p <= split:
            relay(p - 2)
    for p in range(min(split, Z) - 1, split):
        relay(p)
    for p in first:
        norm(p)
    loads[9].wait()
    loads[10].wait()
    steps = [later(arrive, p) for p in third[:1]] + [later(relay, p) for p in second]
    steps += [later(arrive, p) for p in third[1:2]]
    hidden(first, [(i, step) for i, step in enumerate(steps)])
    loads[11].wait()
    last = len(groups) - 1
    if second:
        for p in second:
            norm(p)
        steps = [later(arrive, p) for p in third[2:]] + [later(relay, p) for p in third[:-2]]
        hidden(second, [(i + 1, step) for i, step in enumerate(steps)])
        down(1, turns[:-1])
    else:
        for p in third[2:]:
            arrive(p)
        for p in third[:-2]:
            relay(p)
    down(0, turns[:-1])
    relay(third[-2])
    if second:
        for d in turns[:-1]:
            pair_sum(1, d)
        down(1, turns[-1:])
    for d in turns[:-1]:
        pair_sum(0, d)
    relay(third[-1])
    for p in third[:-1]:
        norm(p)
    down(0, turns[-1:])
    if second:
        c2(1, 0).wait_recv()
    norm(third[-1])
    steps = [later(send_back, p) for p in back[1]] if second else []
    hidden(third, [(NT - 2, step) for step in steps[:1]])
    down(last, turns[:-1])
    for step in steps[1:]:
        step()
    down_block(last, tp_of(y, oc))
    c2(last, 0).start()
    for d in turns[:-1]:
        pair_sum(last, d)
        y2_own(d)
    down_block(last, t)
    c2(0, 0).wait_recv()
    for p in back[0][:-1]:
        send_back(p)
    c2(last, 0).wait_recv()
    for p in back[-1] + [0]:
        send_back(p)

    others = pl.ds(0, (S - 1) * C)
    remote(rb.at[others], ret.at[others], B, b_r.at[0], sp=peer(1)).wait_recv()

    def gwide(tt, j):
        return pl.ds(pl.multiple_of(tt * W + j * GW, GW), GW)

    def gfold(j):
        return pl.ds(j * GW, GW)

    def gy_send(d, j):
        ref = out.at[:, gwide(t, j)]
        return remote(ref, ref, GY, gy_r.at[seen(d), j], tp=tp_of(yo(d), c))

    def gy_recv(d, j):
        ref = out.at[:, gwide(tp_of(yo(d), c), j)]
        return remote(ref, ref, GY, gy_r.at[d - 1, j], tp=tp_of(yo(d), c))

    def gc_send(d, j):
        ref = out.at[:, gwide(tp_of(yo(d), c), j)]
        return remote(ref, ref, GC, gc_r.at[0], tp=tp_of(y, oc))

    pick0 = picker(slot0).astype(BF16)
    pick1 = picker(slot1).astype(BF16)
    rw0 = column(rw[0:1, :])
    rw1 = column(rw[1:2, :])
    for j in range(NG):
        mix0 = jnp.dot(pick0, ret[:, gfold(j)], preferred_element_type=F32)
        mix1 = jnp.dot(pick1, ret[:, gfold(j)], preferred_element_type=F32)
        out[:, gwide(t, j)] = (
            mixed[:, gfold(j)].astype(F32) + (rw0 * mix0 + rw1 * mix1)
        ).astype(BF16)
        for d in range(1, Y):
            gy_send(d, j).start()
        gc_send(0, j).start()

    @pl.when(me < S - 1)
    def _():
        remote(halo, halo, HALO, halo_r.at[0], sp=me + 1).wait_send()

    def drain(ref, sem):
        remote(ref, ref, sem, sem, tp=tp_of(y, oc)).wait_send()

    drain(rc1, C1)
    drain(sb1.at[pl.ds(0, Y - 1)], Y1)
    drain(ret.at[others], A)
    drain(x_all.at[:, pl.ds(0, (Y - 1) * W)], FY)
    drain(x_all.at[:, pl.ds(0, Y * W)], FC)
    drain(x_all.at[:, pl.ds(0, Y * W)], C2)
    drain(x_all.at[:, pl.ds(0, (Y - 1) * W)], Y2)
    drain(ret.at[others], B)

    for j in range(NG):
        for d in range(1, Y):
            gy_recv(d, j).wait_recv()
            gc_send(d, j).start()
    ours = out.at[:, pl.ds(0, Y * W)]
    remote(ours, ours, GC, gc_r.at[0], tp=tp_of(y, oc)).wait_recv()
    drain(ours, GC)
    drain(out.at[:, pl.ds(0, (Y - 1) * W)], GY)


def per_device(
    S,
    T,
    queries,
    key_rows,
    value_rows,
    sink_logits,
    out_weight,
    residual,
    norm_gain,
    routes,
    route_weights,
    gate_weight,
    up_weight,
    down_weight,
):
    R, D = residual.shape
    HW = queries.shape[1]
    Y = T // CORES
    W = D // T
    C = 2 * R * TOP // S
    FL = gate_weight.shape[2]
    NH = 4 if W % 512 == 0 else 1
    NF = 4 if W % 512 == 0 else 1
    NG = 2 if W % 256 == 0 else 1
    hbm = pl.BlockSpec(memory_space=pl.ANY)
    dma = pltpu.SemaphoreType.DMA
    v = pltpu.VMEM
    return pl.pallas_call(
        functools.partial(kernel, S, T),
        out_shape=v((R, D), BF16),
        in_specs=[hbm] * 12,
        out_specs=pl.BlockSpec(memory_space=v),
        scratch_shapes=[
            v((1, sink_logits.shape[0]), F32),
            v(queries.shape, BF16),
            v(key_rows.shape, BF16),
            v(value_rows.shape, BF16),
            v((R, W), BF16),
            v((1, D), F32),
            v((TOP, R), jnp.int32),
            v((TOP, R), F32),
            v(out_weight.shape, BF16),
            v(gate_weight.shape[1:], BF16),
            v(up_weight.shape[1:], BF16),
            v(down_weight.shape[1:], BF16),
            v((2,) + key_rows.shape, BF16),
            v((R, HW), BF16),
            v((R, D), BF16),
            v((Y, R, W), BF16),
            v((Y, NH, R, W // NH), BF16),
            v((Y, NH, R, W // NH), BF16),
            v((R, W), BF16),
            v((S * C, W), BF16),
            v((S * C, D), BF16),
            v((S * C, D), BF16),
            v((S * C, FL), BF16),
            v((S * C, D), BF16),
            v((Y, S * C, W), BF16),
            v((Y - 1, S * C, W), BF16),
            v((Y - 1, S * C, W), BF16),
            v((S * C, W), BF16),
            v((S * C, W), BF16),
            dma((12,)),
            pltpu.SemaphoreType.REGULAR((max(1, (S - 1).bit_length()),)),
            dma((11,)),
            dma((2,)),
            dma((Y,)),
            dma((Y - 1, NH)),
            dma((S, NF)),
            dma((S, Y - 1, NF)),
            dma((S,)),
            dma((3, Y)),
            dma((S, Y - 1, NF)),
            dma((1,)),
            dma((Y - 1, NG)),
            dma((1,)),
        ],
        compiler_params=pltpu.CompilerParams(
            collective_id=0, has_side_effects=True, vmem_limit_bytes=60 * 1024 * 1024
        ),
        name="layer",
    )(
        sink_logits.reshape(1, -1),
        queries,
        key_rows,
        value_rows,
        residual,
        norm_gain.reshape(1, D),
        routes.T,
        route_weights.T,
        out_weight,
        gate_weight,
        up_weight,
        down_weight,
    )


def solution(mesh):
    placed = (
        P("sp", "tp"),
        P("sp", "tp"),
        P("sp", "tp"),
        P("tp"),
        P("tp", None),
        P("sp", None),
        P(),
        P("sp", None),
        P("sp", None),
        P("sp", None, "tp"),
        P("sp", None, "tp"),
        P("sp", "tp", None),
    )
    return jax.shard_map(
        functools.partial(per_device, mesh.shape["sp"], mesh.shape["tp"]),
        mesh=mesh,
        in_specs=placed,
        out_specs=P("sp", None),
        check_vma=False,
    )
```

```python
import functools

import jax
import jax.numpy as jnp
import numpy as np
from jax import lax
from jax.experimental import pallas as pl
from jax.experimental.pallas import tpu as pltpu
from jax.sharding import PartitionSpec as P

HEAD_DIM = 64
WINDOW = 128
TOP = 2
CORES = 2
F32 = jnp.float32
BF16 = jnp.bfloat16
MESH = pl.DeviceIdType.MESH


def kernel(
    S,
    T,
    sink_hbm,
    q_hbm,
    k_hbm,
    v_hbm,
    res_hbm,
    gain_hbm,
    routes_hbm,
    rw_hbm,
    wo_hbm,
    wg_hbm,
    wu_hbm,
    wd_hbm,
    out,
    sink,
    q,
    k,
    v,
    res,
    gain,
    routes,
    rw,
    wo,
    wg,
    wu,
    wd,
    halo,
    att,
    pp,
    rc1,
    sb1,
    ry1,
    mixed,
    picked,
    x_all,
    xn,
    act,
    yp,
    rc2,
    sb2,
    ry2,
    rb,
    ret,
    w_sem,
    met,
    sent,
    halo_r,
    c1_r,
    y1_r,
    a_r,
    fy_r,
    fc_r,
    c2_r,
    y2_r,
    b_r,
    gy_r,
    gc_r,
):
    R, W = res.shape
    D = W * T
    Y = T // CORES
    H = q.shape[1] // HEAD_DIM
    KV = k.shape[1] // HEAD_DIM
    G = H // KV
    C = x_all.shape[0] // S
    Z = S // 2
    FL = wg.shape[1]
    NH = y1_r.shape[1]
    HALO, C1, Y1, A, FY, FC, C2, Y2, B, GY, GC = (sent.at[i] for i in range(11))
    HW = W // NH
    NF = a_r.shape[1]
    NG = gy_r.shape[1]
    GW = W // NG
    NB = y2_r.shape[2]
    BW = W // NB
    FW = W // NF

    me = lax.axis_index("sp")
    t = lax.axis_index("tp")
    y = t // CORES
    c = t % CORES
    oc = 1 - c
    z = me // 2
    x = me % 2

    def tp_of(yy, cc):
        return yy * CORES + cc

    def cols(tt):
        return pl.ds(pl.multiple_of(tt * W, W), W)

    def part(tt, j):
        return pl.ds(pl.multiple_of(tt * W + j * HW, HW), HW)

    def wide(tt, f):
        return pl.ds(pl.multiple_of(tt * W + f * FW, FW), FW)

    def fold(f):
        return pl.ds(f * FW, FW)

    def rows(s):
        return pl.ds(pl.multiple_of(s * C, C), C)

    def yo(d):
        return (y + d) % Y

    def seen(d):
        return Y - d - 1

    def remote(src, dst, ss, rs, **dev):
        return pltpu.make_async_remote_copy(
            src_ref=src, dst_ref=dst, send_sem=ss, recv_sem=rs, device_id=dev, device_id_type=MESH
        )

    places = [(0, 0), (1, 0)] + [(0, d) for d in range(1, Z)] + [(1, d) for d in range(1, Z)]
    split = min(3, Z + 1)
    first = list(range(split))
    second = list(range(split, Z + 1))
    third = list(range(Z + 1, S))

    def peer(p):
        parity, bits = places[p]
        zz = z
        bit = 1
        while bit < Z:
            if bits // bit % 2:
                zz = zz + bit * (1 - 2 * (zz // bit % 2))
            bit *= 2
        return 2 * zz + (x + parity) % 2

    def span(p):
        return pl.ds(p * C, C)

    def block(group):
        return pl.ds(group[0] * C, len(group) * C)

    barrier = pltpu.get_barrier_semaphore()

    def greet(sem, step):
        for ok, e in ((me >= step, me - step), (me + step < S, me + step)):

            @pl.when(ok)
            def _(e=e):
                pl.semaphore_signal(sem, inc=1, device_id={"sp": e}, device_id_type=MESH)

    def greeted(sem, step, more=0):
        both = jnp.minimum(me // step, 1) + jnp.minimum((S - 1 - me) // step, 1)
        pl.semaphore_wait(sem, both + more)

    reach = [1]
    while 2 * reach[-1] < S:
        reach.append(2 * reach[-1])

    def meet(i):
        if i:
            greeted(met.at[i - 1], reach[i - 1])
        if i < len(reach):
            greet(met.at[i], reach[i])

    greet(barrier, 1)
    for d in range(1, Y):
        pl.semaphore_signal(
            barrier, inc=1, device_id={"tp": tp_of(yo(d), c)}, device_id_type=MESH
        )
    pl.semaphore_signal(barrier, inc=1, device_id={"tp": tp_of(y, oc)}, device_id_type=MESH)

    loads = [
        pltpu.make_async_copy(src, dst, w_sem.at[i])
        for i, (src, dst) in enumerate(
            (
                (k_hbm, k),
                (v_hbm, v),
                (q_hbm, q),
                (routes_hbm, routes),
                (sink_hbm, sink),
                (res_hbm.at[:, cols(t)], res),
                (rw_hbm, rw),
                (gain_hbm, gain),
                (wo_hbm, wo),
                (wg_hbm.at[0], wg),
                (wu_hbm.at[0], wu),
                (wd_hbm.at[0], wd),
            )
        )
    ]
    for load in loads:
        load.start()
    loads[0].wait()
    loads[1].wait()
    greeted(barrier, 1, Y)

    halo_copies = [
        remote(src, halo.at[i], HALO, halo_r.at[i], sp=jnp.minimum(me + 1, S - 1))
        for i, src in enumerate((k, v))
    ]

    @pl.when(me < S - 1)
    def _():
        for copy in halo_copies:
            copy.start()

    meet(0)
    for load in loads[2:5]:
        load.wait()

    qi = lax.broadcasted_iota(jnp.int32, (R, R), 0)
    kj = lax.broadcasted_iota(jnp.int32, (R, R), 1)
    dist_own = (qi - kj).astype(F32)
    dist_old = (qi - kj + WINDOW).astype(F32)
    nt = (((1,), (1,)), ((), ()))

    ok_own = qi >= kj
    ok_old = (kj >= qi) & (kj + me * R >= WINDOW)

    base = jnp.float32(1.0)
    for i in range(1, T):
        base = jnp.where(t == i, jnp.float32(2.0 ** (-8.0 * i / T)), base)

    def head(h):
        return slice(h * HEAD_DIM, (h + 1) * HEAD_DIM), slice(
            (h // G) * HEAD_DIM, (h // G + 1) * HEAD_DIM
        )

    def scores(h, keys, dist, ok):
        raw = lax.dot_general(q[:, head(h)[0]], keys, nt, preferred_element_type=F32)
        slope = base * np.float32(2.0 ** (-8.0 * (h + 1) / (H * T)))
        return jnp.where(ok, raw * HEAD_DIM**-0.5 - slope * dist, -jnp.inf)

    s_own = [scores(h, k[:, head(h)[1]], dist_own, ok_own) for h in range(H)]
    top = [jnp.max(a, axis=1, keepdims=True) for a in s_own]
    e_own = [jnp.exp(a - b) for a, b in zip(s_own, top)]
    weight = [jnp.sum(a, axis=1, keepdims=True) for a in e_own]
    mix_own = [
        jnp.dot(a.astype(BF16), v[:, head(h)[1]], preferred_element_type=F32)
        for h, a in enumerate(e_own)
    ]

    meet(1)

    def column(row):
        return jnp.broadcast_to(row, (R, R)).T[:, 0:1]

    r0 = column(routes[0:1, :].astype(F32)).astype(jnp.int32)
    r1 = column(routes[1:2, :].astype(F32)).astype(jnp.int32)
    lane_e = lax.broadcasted_iota(jnp.int32, (R, 128), 1)
    hit0 = lane_e == r0
    hit1 = lane_e == r1
    member = jnp.where(hit0 | hit1, 1.0, 0.0).astype(BF16)
    tri = jnp.where(
        lax.broadcasted_iota(jnp.int32, (R, R), 1) < lax.broadcasted_iota(jnp.int32, (R, R), 0),
        1.0,
        0.0,
    ).astype(BF16)
    rank = jnp.dot(tri, member, preferred_element_type=F32)
    rank0 = jnp.sum(jnp.where(hit0, rank, 0.0), axis=1, keepdims=True)
    rank1 = jnp.sum(jnp.where(hit1, rank, 0.0), axis=1, keepdims=True)
    slot0 = r0.astype(F32) * C + rank0
    slot1 = r1.astype(F32) * C + rank1
    lane_s = lax.broadcasted_iota(jnp.int32, (R, S * C), 1).astype(F32)

    def picker(slot):
        return jnp.where(lane_s == slot, 1.0, 0.0)

    both = (picker(slot0) + picker(slot1)).T.astype(BF16)

    @pl.when(me > 0)
    def _():
        halo_copies[0].wait_recv()

    @pl.when(me == 0)
    def _():
        halo[...] = jnp.zeros_like(halo)

    s_old = [scores(h, halo[0, :, head(h)[1]], dist_old, ok_old) for h in range(H)]
    peak = [jnp.maximum(a, jnp.max(b, axis=1, keepdims=True)) for a, b in zip(top, s_old)]
    shrink = [jnp.exp(a - b) for a, b in zip(top, peak)]
    e_old = [jnp.exp(a - b) for a, b in zip(s_old, peak)]
    total = [
        a * b + jnp.sum(e, axis=1, keepdims=True) for a, b, e in zip(weight, shrink, e_old)
    ]
    keep = [
        1.0 / (a + jnp.exp(sink[0:1, h : h + 1] - b)) for h, (a, b) in enumerate(zip(total, peak))
    ]

    @pl.when(me > 0)
    def _():
        halo_copies[1].wait_recv()

    mix_old = [
        jnp.dot(a.astype(BF16), halo[1, :, head(h)[1]], preferred_element_type=F32)
        for h, a in enumerate(e_old)
    ]
    for h in range(H):
        att[:, head(h)[0]] = ((mix_own[h] * shrink[h] + mix_old[h]) * keep[h]).astype(BF16)

    meet(2)
    for load in loads[5:9]:
        load.wait()

    def project(tt):
        pp[:, cols(tt)] = jnp.dot(att[...], wo[:, cols(tt)], preferred_element_type=F32).astype(
            BF16
        )

    def c1(yy):
        return remote(
            pp.at[:, cols(tp_of(yy, oc))], rc1.at[yy], C1, c1_r.at[yy], tp=tp_of(y, oc)
        )

    def y1_send(d, j):
        yy = yo(d)
        return remote(
            sb1.at[yy, j], ry1.at[y, j], Y1, y1_r.at[seen(d), j], tp=tp_of(yy, c)
        )

    def y1_recv(d, j):
        yy = yo(d)
        return remote(sb1.at[yy, j], ry1.at[yy, j], Y1, y1_r.at[d - 1, j], tp=tp_of(yy, c))

    turns = list(range(1, Y)) + [0]

    def half(j):
        return slice(j * HW, (j + 1) * HW)

    for d in turns[:-1]:
        project(tp_of(yo(d), oc))
        c1(yo(d)).start()
    for d in turns[:-1]:
        project(tp_of(yo(d), c))
    for d in turns[:-1]:
        c1(yo(d)).wait_recv()
        for j in range(NH):
            sb1[yo(d), j] = (
                pp[:, part(tp_of(yo(d), c), j)].astype(F32) + rc1[yo(d), :, half(j)].astype(F32)
            ).astype(BF16)
            y1_send(d, j).start()
    project(tp_of(y, oc))
    c1(y).start()
    project(t)
    c1(y).wait_recv()
    for i in range(3, len(reach) + 1):
        meet(i)

    def a_send(p, j):
        e = peer(p)
        return remote(
            picked.at[rows(e), half(j)],
            x_all.at[span(p), part(t, j)],
            A,
            a_r.at[p, j * NF // NH],
            sp=e,
        )

    def a_fold(p, f):
        e = peer(p)
        return remote(
            picked.at[rows(e), fold(f)], x_all.at[span(p), wide(t, f)], A, a_r.at[p, f], sp=e
        )

    def fy_send(p, d, f):
        ref = x_all.at[span(p), wide(t, f)]
        return remote(ref, ref, FY, fy_r.at[p, seen(d)], tp=tp_of(yo(d), c))

    def fy_recv(p, d):
        ref = x_all.at[span(p), cols(tp_of(yo(d), c))]
        return remote(ref, ref, FY, fy_r.at[p, d - 1], tp=tp_of(yo(d), c))

    def fc_send(p, d):
        ref = x_all.at[span(p), cols(tp_of(yo(d), c))]
        return remote(ref, ref, FC, fc_r.at[p], tp=tp_of(y, oc))

    def fc_recv(p):
        ref = x_all.at[span(p), pl.ds(0, Y * W)]
        return remote(ref, ref, FC, fc_r.at[p], tp=tp_of(y, oc))

    arrivals = list(range(1, Z + 1))

    for j in range(NH):
        head_sum = pp[:, part(t, j)].astype(F32) + rc1[y, :, half(j)].astype(F32)
        for d in range(1, Y):
            y1_recv(d, j).wait_recv()
            head_sum = head_sum + ry1[yo(d), j].astype(F32)
        mixed[:, half(j)] = (res[:, half(j)].astype(F32) + head_sum).astype(BF16)
        picked[:, half(j)] = jnp.dot(
            both, mixed[:, half(j)], preferred_element_type=F32
        ).astype(BF16)
        for p in arrivals:
            a_send(p, j).start()
    for f in range(NF):
        a_fold(third[0], f).start()
    x_all[span(0), cols(t)] = picked[rows(me)]

    def forward(p, f):
        for d in range(1, Y):
            fy_send(p, d, f).start()

    def relay(p):
        for d in range(1, Y):
            fy_recv(p, d).wait_recv()
            fc_send(p, d).start()

    def arrive(p):
        for f in range(NF):
            a_fold(p, f).wait_recv()
            forward(p, f)
        fc_send(p, 0).start()

    def norm(p):
        fc_recv(p).wait_recv()
        wide = x_all[span(p)].astype(F32)
        scale = lax.rsqrt(jnp.mean(wide * wide, axis=1, keepdims=True) + 1e-06)
        xn[span(p)] = (wide * scale * gain[...]).astype(BF16)

    TN = min(256, FL)
    NT = FL // TN

    def hidden(group, hooks):
        at = block(group)

        @pl.loop(0, NT)
        def _(n):
            nn = pl.ds(pl.multiple_of(n * TN, TN), TN)
            gate = jnp.dot(xn[at], wg[:, nn], preferred_element_type=F32)
            up = jnp.dot(xn[at], wu[:, nn], preferred_element_type=F32)
            act[at, nn] = (gate / (1.0 + jnp.exp(-gate)) * up).astype(BF16)
            for i in range(NT):
                todo = [hook for turn, hook in hooks if min(turn, NT - 1) == i]
                if todo:

                    @pl.when(n == i)
                    def _(todo=todo):
                        for hook in todo:
                            hook()

    def c2(g, d):
        at = block(groups[g])
        return remote(
            yp.at[at, cols(tp_of(yo(d), oc))], rc2.at[d, at], C2, c2_r.at[g, d], tp=tp_of(y, oc)
        )

    def down_block(g, tt):
        at = block(groups[g])
        yp[at, cols(tt)] = jnp.dot(act[at], wd[:, cols(tt)], preferred_element_type=F32).astype(
            BF16
        )

    def bwide(tt, f):
        return pl.ds(pl.multiple_of(tt * W + f * BW, BW), BW)

    def bfold(f):
        return pl.ds(f * BW, BW)

    def y2_send(p, d, f):
        return remote(
            sb2.at[d - 1, span(p), bfold(f)],
            ry2.at[seen(d), span(p), bfold(f)],
            Y2,
            y2_r.at[p, seen(d), f],
            tp=tp_of(yo(d), c),
        )

    def y2_recv(p, d, f):
        return remote(
            sb2.at[d - 1, span(p), bfold(f)],
            ry2.at[d - 1, span(p), bfold(f)],
            Y2,
            y2_r.at[p, d - 1, f],
            tp=tp_of(yo(d), c),
        )

    groups = [g for g in (first, second, third) if g]
    back = [g[:0:-1] + g[:1] if g is first else g[1:] + g[:1] for g in groups]

    def pair_sum(g, d):
        c2(g, d).wait_recv()
        for p in back[g]:
            at = span(p)
            sb2[d - 1, at] = (
                yp[at, cols(tp_of(yo(d), c))].astype(F32) + rc2[d, at].astype(F32)
            ).astype(BF16)
            if p:
                for f in range(NB):
                    y2_send(p, d, f).start()

    def y2_own(d):
        for f in range(NB):
            y2_send(0, d, f).start()

    def down(g, turn):
        for d in turn:
            down_block(g, tp_of(yo(d), oc))
            c2(g, d).start()
        for d in turn:
            down_block(g, tp_of(yo(d), c))

    def b_send(p, f):
        e = peer(p)
        return remote(
            rb.at[span(p), bfold(f)], ret.at[rows(me), bfold(f)], B, b_r.at[0], sp=e
        )

    def send_back(p):
        at = span(p)
        for f in range(NB):
            total = yp[at, bwide(t, f)].astype(F32) + rc2[0, at, bfold(f)].astype(F32)
            for d in range(1, Y):
                y2_recv(p, d, f).wait_recv()
                total = total + ry2[d - 1, at, bfold(f)].astype(F32)
            if p:
                rb[at, bfold(f)] = total.astype(BF16)
                b_send(p, f).start()
            else:
                ret[rows(me), bfold(f)] = total.astype(BF16)

    def later(f, *args):
        return lambda: f(*args)

    for f in range(NF):
        forward(0, f)
    fc_send(0, 0).start()
    for i, p in enumerate(arrivals):
        arrive(p)
        if i == 1:
            for q in third[1:]:
                for f in range(NF):
                    a_fold(q, f).start()
        if 1 <= i and p <= split:
            relay(p - 2)
    for p in range(min(split, Z) - 1, split):
        relay(p)
    for p in first:
        norm(p)
    loads[9].wait()
    loads[10].wait()
    steps = [later(arrive, p) for p in third[:1]] + [later(relay, p) for p in second]
    steps += [later(arrive, p) for p in third[1:2]]
    hidden(first, [(i, step) for i, step in enumerate(steps)])
    loads[11].wait()
    last = len(groups) - 1
    if second:
        for p in second:
            norm(p)
        steps = [later(arrive, p) for p in third[2:]] + [later(relay, p) for p in third[:-2]]
        hidden(second, [(i + 1, step) for i, step in enumerate(steps)])
        down(1, turns[:-1])
    else:
        for p in third[2:]:
            arrive(p)
        for p in third[:-2]:
            relay(p)
    down(0, turns[:-1])
    relay(third[-2])
    if second:
        for d in turns[:-1]:
            pair_sum(1, d)
        down(1, turns[-1:])
    for d in turns[:-1]:
        pair_sum(0, d)
    relay(third[-1])
    for p in third[:-1]:
        norm(p)
    down(0, turns[-1:])
    if second:
        c2(1, 0).wait_recv()
    norm(third[-1])
    steps = [later(send_back, p) for p in back[1]] if second else []
    hidden(third, [(NT - 2, step) for step in steps[:1]])
    down(last, turns[:-1])
    for step in steps[1:]:
        step()
    down_block(last, tp_of(y, oc))
    c2(last, 0).start()
    for d in turns[:-1]:
        pair_sum(last, d)
        y2_own(d)
    down_block(last, t)
    c2(0, 0).wait_recv()
    for p in back[0][:-1]:
        send_back(p)
    c2(last, 0).wait_recv()
    for p in back[-1] + [0]:
        send_back(p)

    others = pl.ds(0, (S - 1) * C)
    remote(rb.at[others], ret.at[others], B, b_r.at[0], sp=peer(1)).wait_recv()

    def gwide(tt, j):
        return pl.ds(pl.multiple_of(tt * W + j * GW, GW), GW)

    def gfold(j):
        return pl.ds(j * GW, GW)

    def gy_send(d, j):
        ref = out.at[:, gwide(t, j)]
        return remote(ref, ref, GY, gy_r.at[seen(d), j], tp=tp_of(yo(d), c))

    def gy_recv(d, j):
        ref = out.at[:, gwide(tp_of(yo(d), c), j)]
        return remote(ref, ref, GY, gy_r.at[d - 1, j], tp=tp_of(yo(d), c))

    def gc_send(d, j):
        ref = out.at[:, gwide(tp_of(yo(d), c), j)]
        return remote(ref, ref, GC, gc_r.at[0], tp=tp_of(y, oc))

    pick0 = picker(slot0).astype(BF16)
    pick1 = picker(slot1).astype(BF16)
    rw0 = column(rw[0:1, :])
    rw1 = column(rw[1:2, :])
    for j in range(NG):
        mix0 = jnp.dot(pick0, ret[:, gfold(j)], preferred_element_type=F32)
        mix1 = jnp.dot(pick1, ret[:, gfold(j)], preferred_element_type=F32)
        out[:, gwide(t, j)] = (
            mixed[:, gfold(j)].astype(F32) + (rw0 * mix0 + rw1 * mix1)
        ).astype(BF16)
        for d in range(1, Y):
            gy_send(d, j).start()
        gc_send(0, j).start()

    @pl.when(me < S - 1)
    def _():
        remote(halo, halo, HALO, halo_r.at[0], sp=me + 1).wait_send()

    def drain(ref, sem):
        remote(ref, ref, sem, sem, tp=tp_of(y, oc)).wait_send()

    drain(rc1, C1)
    drain(sb1.at[pl.ds(0, Y - 1)], Y1)
    drain(ret.at[others], A)
    drain(x_all.at[:, pl.ds(0, (Y - 1) * W)], FY)
    drain(x_all.at[:, pl.ds(0, Y * W)], FC)
    drain(x_all.at[:, pl.ds(0, Y * W)], C2)
    drain(x_all.at[:, pl.ds(0, (Y - 1) * W)], Y2)
    drain(ret.at[others], B)

    for j in range(NG):
        for d in range(1, Y):
            gy_recv(d, j).wait_recv()
            gc_send(d, j).start()
    ours = out.at[:, pl.ds(0, Y * W)]
    remote(ours, ours, GC, gc_r.at[0], tp=tp_of(y, oc)).wait_recv()
    drain(ours, GC)
    drain(out.at[:, pl.ds(0, (Y - 1) * W)], GY)


def per_device(
    S,
    T,
    queries,
    key_rows,
    value_rows,
    sink_logits,
    out_weight,
    residual,
    norm_gain,
    routes,
    route_weights,
    gate_weight,
    up_weight,
    down_weight,
):
    R, D = residual.shape
    HW = queries.shape[1]
    Y = T // CORES
    W = D // T
    C = 2 * R * TOP // S
    FL = gate_weight.shape[2]
    NH = 4 if W % 512 == 0 else 1
    NF = 2 if W % 256 == 0 else 1
    NG = 2 if W % 256 == 0 else 1
    NB = 2 if W % 256 == 0 else 1
    hbm = pl.BlockSpec(memory_space=pl.ANY)
    dma = pltpu.SemaphoreType.DMA
    v = pltpu.VMEM
    return pl.pallas_call(
        functools.partial(kernel, S, T),
        out_shape=v((R, D), BF16),
        in_specs=[hbm] * 12,
        out_specs=pl.BlockSpec(memory_space=v),
        scratch_shapes=[
            v((1, sink_logits.shape[0]), F32),
            v(queries.shape, BF16),
            v(key_rows.shape, BF16),
            v(value_rows.shape, BF16),
            v((R, W), BF16),
            v((1, D), F32),
            v((TOP, R), jnp.int32),
            v((TOP, R), F32),
            v(out_weight.shape, BF16),
            v(gate_weight.shape[1:], BF16),
            v(up_weight.shape[1:], BF16),
            v(down_weight.shape[1:], BF16),
            v((2,) + key_rows.shape, BF16),
            v((R, HW), BF16),
            v((R, D), BF16),
            v((Y, R, W), BF16),
            v((Y, NH, R, W // NH), BF16),
            v((Y, NH, R, W // NH), BF16),
            v((R, W), BF16),
            v((S * C, W), BF16),
            v((S * C, D), BF16),
            v((S * C, D), BF16),
            v((S * C, FL), BF16),
            v((S * C, D), BF16),
            v((Y, S * C, W), BF16),
            v((Y - 1, S * C, W), BF16),
            v((Y - 1, S * C, W), BF16),
            v((S * C, W), BF16),
            v((S * C, W), BF16),
            dma((12,)),
            pltpu.SemaphoreType.REGULAR((max(1, (S - 1).bit_length()),)),
            dma((11,)),
            dma((2,)),
            dma((Y,)),
            dma((Y - 1, NH)),
            dma((S, NF)),
            dma((S, Y - 1)),
            dma((S,)),
            dma((3, Y)),
            dma((S, Y - 1, NB)),
            dma((1,)),
            dma((Y - 1, NG)),
            dma((1,)),
        ],
        compiler_params=pltpu.CompilerParams(
            collective_id=0, has_side_effects=True, vmem_limit_bytes=60 * 1024 * 1024
        ),
        name="layer",
    )(
        sink_logits.reshape(1, -1),
        queries,
        key_rows,
        value_rows,
        residual,
        norm_gain.reshape(1, D),
        routes.T,
        route_weights.T,
        out_weight,
        gate_weight,
        up_weight,
        down_weight,
    )


def solution(mesh):
    placed = (
        P("sp", "tp"),
        P("sp", "tp"),
        P("sp", "tp"),
        P("tp"),
        P("tp", None),
        P("sp", None),
        P(),
        P("sp", None),
        P("sp", None),
        P("sp", None, "tp"),
        P("sp", None, "tp"),
        P("sp", "tp", None),
    )
    return jax.shard_map(
        functools.partial(per_device, mesh.shape["sp"], mesh.shape["tp"]),
        mesh=mesh,
        in_specs=placed,
        out_specs=P("sp", None),
        check_vma=False,
    )
```

```python
import functools

import jax
import jax.numpy as jnp
import numpy as np
from jax import lax
from jax.experimental import pallas as pl
from jax.experimental.pallas import tpu as pltpu
from jax.sharding import PartitionSpec as P

HEAD_DIM = 64
WINDOW = 128
TOP = 2
CORES = 2
F32 = jnp.float32
BF16 = jnp.bfloat16
MESH = pl.DeviceIdType.MESH


def kernel(
    S,
    T,
    sink_hbm,
    q_hbm,
    k_hbm,
    v_hbm,
    res_hbm,
    gain_hbm,
    routes_hbm,
    rw_hbm,
    wo_hbm,
    wg_hbm,
    wu_hbm,
    wd_hbm,
    out,
    sink,
    q,
    k,
    v,
    res,
    gain,
    routes,
    rw,
    wo,
    wg,
    wu,
    wd,
    halo,
    att,
    pp,
    rc1,
    sb1,
    ry1,
    mixed,
    picked,
    x_all,
    xn,
    act,
    yp,
    rc2,
    sb2,
    ry2,
    rb,
    ret,
    w_sem,
    met,
    sent,
    halo_r,
    c1_r,
    y1_r,
    a_r,
    fy_r,
    fc_r,
    c2_r,
    y2_r,
    b_r,
    gy_r,
    gc_r,
):
    R, W = res.shape
    D = W * T
    Y = T // CORES
    H = q.shape[1] // HEAD_DIM
    KV = k.shape[1] // HEAD_DIM
    G = H // KV
    C = x_all.shape[0] // S
    Z = S // 2
    FL = wg.shape[1]
    NH = y1_r.shape[1]
    HALO, C1, Y1, A, FY, FC, C2, Y2, B, GY, GC = (sent.at[i] for i in range(11))
    HW = W // NH
    NF = a_r.shape[1]
    NG = gy_r.shape[1]
    GW = W // NG
    NB = y2_r.shape[2]
    BW = W // NB
    FW = W // NF

    me = lax.axis_index("sp")
    t = lax.axis_index("tp")
    y = t // CORES
    c = t % CORES
    oc = 1 - c
    z = me // 2
    x = me % 2

    def tp_of(yy, cc):
        return yy * CORES + cc

    def cols(tt):
        return pl.ds(pl.multiple_of(tt * W, W), W)

    def part(tt, j):
        return pl.ds(pl.multiple_of(tt * W + j * HW, HW), HW)

    def wide(tt, f):
        return pl.ds(pl.multiple_of(tt * W + f * FW, FW), FW)

    def fold(f):
        return pl.ds(f * FW, FW)

    def rows(s):
        return pl.ds(pl.multiple_of(s * C, C), C)

    def yo(d):
        return (y + d) % Y

    def seen(d):
        return Y - d - 1

    def remote(src, dst, ss, rs, **dev):
        return pltpu.make_async_remote_copy(
            src_ref=src, dst_ref=dst, send_sem=ss, recv_sem=rs, device_id=dev, device_id_type=MESH
        )

    places = [(0, 0), (1, 0)] + [(0, d) for d in range(1, Z)] + [(1, d) for d in range(1, Z)]
    split = min(3, Z + 1)
    first = list(range(split))
    second = list(range(split, Z + 1))
    third = list(range(Z + 1, S))

    def peer(p):
        parity, bits = places[p]
        zz = z
        bit = 1
        while bit < Z:
            if bits // bit % 2:
                zz = zz + bit * (1 - 2 * (zz // bit % 2))
            bit *= 2
        return 2 * zz + (x + parity) % 2

    def span(p):
        return pl.ds(p * C, C)

    def block(group):
        return pl.ds(group[0] * C, len(group) * C)

    barrier = pltpu.get_barrier_semaphore()

    def greet(sem, step):
        for ok, e in ((me >= step, me - step), (me + step < S, me + step)):

            @pl.when(ok)
            def _(e=e):
                pl.semaphore_signal(sem, inc=1, device_id={"sp": e}, device_id_type=MESH)

    def greeted(sem, step, more=0):
        both = jnp.minimum(me // step, 1) + jnp.minimum((S - 1 - me) // step, 1)
        pl.semaphore_wait(sem, both + more)

    reach = [1]
    while 2 * reach[-1] < S:
        reach.append(2 * reach[-1])

    def meet(i):
        if i:
            greeted(met.at[i - 1], reach[i - 1])
        if i < len(reach):
            greet(met.at[i], reach[i])

    greet(barrier, 1)
    for d in range(1, Y):
        pl.semaphore_signal(
            barrier, inc=1, device_id={"tp": tp_of(yo(d), c)}, device_id_type=MESH
        )
    pl.semaphore_signal(barrier, inc=1, device_id={"tp": tp_of(y, oc)}, device_id_type=MESH)

    loads = [
        pltpu.make_async_copy(src, dst, w_sem.at[i])
        for i, (src, dst) in enumerate(
            (
                (k_hbm, k),
                (v_hbm, v),
                (q_hbm, q),
                (routes_hbm, routes),
                (sink_hbm, sink),
                (res_hbm.at[:, cols(t)], res),
                (rw_hbm, rw),
                (gain_hbm, gain),
                (wo_hbm, wo),
                (wg_hbm.at[0], wg),
                (wu_hbm.at[0], wu),
                (wd_hbm.at[0], wd),
            )
        )
    ]
    for load in loads[:8]:
        load.start()
    loads[0].wait()
    loads[1].wait()
    greeted(barrier, 1, Y)

    halo_copies = [
        remote(src, halo.at[i], HALO, halo_r.at[i], sp=jnp.minimum(me + 1, S - 1))
        for i, src in enumerate((k, v))
    ]

    @pl.when(me < S - 1)
    def _():
        for copy in halo_copies:
            copy.start()

    meet(0)
    for load in loads[8:]:
        load.start()
    for load in loads[2:5]:
        load.wait()

    qi = lax.broadcasted_iota(jnp.int32, (R, R), 0)
    kj = lax.broadcasted_iota(jnp.int32, (R, R), 1)
    dist_own = (qi - kj).astype(F32)
    dist_old = (qi - kj + WINDOW).astype(F32)
    nt = (((1,), (1,)), ((), ()))

    ok_own = qi >= kj
    ok_old = (kj >= qi) & (kj + me * R >= WINDOW)

    base = jnp.float32(1.0)
    for i in range(1, T):
        base = jnp.where(t == i, jnp.float32(2.0 ** (-8.0 * i / T)), base)

    def head(h):
        return slice(h * HEAD_DIM, (h + 1) * HEAD_DIM), slice(
            (h // G) * HEAD_DIM, (h // G + 1) * HEAD_DIM
        )

    def scores(h, keys, dist, ok):
        raw = lax.dot_general(q[:, head(h)[0]], keys, nt, preferred_element_type=F32)
        slope = base * np.float32(2.0 ** (-8.0 * (h + 1) / (H * T)))
        return jnp.where(ok, raw * HEAD_DIM**-0.5 - slope * dist, -jnp.inf)

    s_own = [scores(h, k[:, head(h)[1]], dist_own, ok_own) for h in range(H)]
    top = [jnp.max(a, axis=1, keepdims=True) for a in s_own]
    e_own = [jnp.exp(a - b) for a, b in zip(s_own, top)]
    weight = [jnp.sum(a, axis=1, keepdims=True) for a in e_own]
    mix_own = [
        jnp.dot(a.astype(BF16), v[:, head(h)[1]], preferred_element_type=F32)
        for h, a in enumerate(e_own)
    ]

    meet(1)

    def column(row):
        return jnp.broadcast_to(row, (R, R)).T[:, 0:1]

    r0 = column(routes[0:1, :].astype(F32)).astype(jnp.int32)
    r1 = column(routes[1:2, :].astype(F32)).astype(jnp.int32)
    lane_e = lax.broadcasted_iota(jnp.int32, (R, 128), 1)
    hit0 = lane_e == r0
    hit1 = lane_e == r1
    member = jnp.where(hit0 | hit1, 1.0, 0.0).astype(BF16)
    tri = jnp.where(
        lax.broadcasted_iota(jnp.int32, (R, R), 1) < lax.broadcasted_iota(jnp.int32, (R, R), 0),
        1.0,
        0.0,
    ).astype(BF16)
    rank = jnp.dot(tri, member, preferred_element_type=F32)
    rank0 = jnp.sum(jnp.where(hit0, rank, 0.0), axis=1, keepdims=True)
    rank1 = jnp.sum(jnp.where(hit1, rank, 0.0), axis=1, keepdims=True)
    slot0 = r0.astype(F32) * C + rank0
    slot1 = r1.astype(F32) * C + rank1
    lane_s = lax.broadcasted_iota(jnp.int32, (R, S * C), 1).astype(F32)

    def picker(slot):
        return jnp.where(lane_s == slot, 1.0, 0.0)

    both = (picker(slot0) + picker(slot1)).T.astype(BF16)

    @pl.when(me > 0)
    def _():
        halo_copies[0].wait_recv()

    @pl.when(me == 0)
    def _():
        halo[...] = jnp.zeros_like(halo)

    s_old = [scores(h, halo[0, :, head(h)[1]], dist_old, ok_old) for h in range(H)]
    peak = [jnp.maximum(a, jnp.max(b, axis=1, keepdims=True)) for a, b in zip(top, s_old)]
    shrink = [jnp.exp(a - b) for a, b in zip(top, peak)]
    e_old = [jnp.exp(a - b) for a, b in zip(s_old, peak)]
    total = [
        a * b + jnp.sum(e, axis=1, keepdims=True) for a, b, e in zip(weight, shrink, e_old)
    ]
    keep = [
        1.0 / (a + jnp.exp(sink[0:1, h : h + 1] - b)) for h, (a, b) in enumerate(zip(total, peak))
    ]

    @pl.when(me > 0)
    def _():
        halo_copies[1].wait_recv()

    mix_old = [
        jnp.dot(a.astype(BF16), halo[1, :, head(h)[1]], preferred_element_type=F32)
        for h, a in enumerate(e_old)
    ]
    for h in range(H):
        att[:, head(h)[0]] = ((mix_own[h] * shrink[h] + mix_old[h]) * keep[h]).astype(BF16)

    meet(2)
    for load in loads[5:9]:
        load.wait()

    def project(tt):
        pp[:, cols(tt)] = jnp.dot(att[...], wo[:, cols(tt)], preferred_element_type=F32).astype(
            BF16
        )

    def c1(yy):
        return remote(
            pp.at[:, cols(tp_of(yy, oc))], rc1.at[yy], C1, c1_r.at[yy], tp=tp_of(y, oc)
        )

    def y1_send(d, j):
        yy = yo(d)
        return remote(
            sb1.at[yy, j], ry1.at[y, j], Y1, y1_r.at[seen(d), j], tp=tp_of(yy, c)
        )

    def y1_recv(d, j):
        yy = yo(d)
        return remote(sb1.at[yy, j], ry1.at[yy, j], Y1, y1_r.at[d - 1, j], tp=tp_of(yy, c))

    turns = list(range(1, Y)) + [0]

    def half(j):
        return slice(j * HW, (j + 1) * HW)

    for d in turns[:-1]:
        project(tp_of(yo(d), oc))
        c1(yo(d)).start()
    for d in turns[:-1]:
        project(tp_of(yo(d), c))
    for d in turns[:-1]:
        c1(yo(d)).wait_recv()
        for j in range(NH):
            sb1[yo(d), j] = (
                pp[:, part(tp_of(yo(d), c), j)].astype(F32) + rc1[yo(d), :, half(j)].astype(F32)
            ).astype(BF16)
            y1_send(d, j).start()
    project(tp_of(y, oc))
    c1(y).start()
    project(t)
    c1(y).wait_recv()
    for i in range(3, len(reach) + 1):
        meet(i)

    def a_send(p, j):
        e = peer(p)
        return remote(
            picked.at[rows(e), half(j)],
            x_all.at[span(p), part(t, j)],
            A,
            a_r.at[p, j * NF // NH],
            sp=e,
        )

    def a_fold(p, f):
        e = peer(p)
        return remote(
            picked.at[rows(e), fold(f)], x_all.at[span(p), wide(t, f)], A, a_r.at[p, f], sp=e
        )

    def fy_send(p, d, f):
        ref = x_all.at[span(p), wide(t, f)]
        return remote(ref, ref, FY, fy_r.at[p, seen(d)], tp=tp_of(yo(d), c))

    def fy_recv(p, d):
        ref = x_all.at[span(p), cols(tp_of(yo(d), c))]
        return remote(ref, ref, FY, fy_r.at[p, d - 1], tp=tp_of(yo(d), c))

    def fc_send(p, d):
        ref = x_all.at[span(p), cols(tp_of(yo(d), c))]
        return remote(ref, ref, FC, fc_r.at[p], tp=tp_of(y, oc))

    def fc_recv(p):
        ref = x_all.at[span(p), pl.ds(0, Y * W)]
        return remote(ref, ref, FC, fc_r.at[p], tp=tp_of(y, oc))

    arrivals = list(range(1, Z + 1))

    for j in range(NH):
        head_sum = pp[:, part(t, j)].astype(F32) + rc1[y, :, half(j)].astype(F32)
        for d in range(1, Y):
            y1_recv(d, j).wait_recv()
            head_sum = head_sum + ry1[yo(d), j].astype(F32)
        mixed[:, half(j)] = (res[:, half(j)].astype(F32) + head_sum).astype(BF16)
        picked[:, half(j)] = jnp.dot(
            both, mixed[:, half(j)], preferred_element_type=F32
        ).astype(BF16)
        for p in arrivals:
            a_send(p, j).start()
    for f in range(NF):
        a_fold(third[0], f).start()
    x_all[span(0), cols(t)] = picked[rows(me)]

    def forward(p, f):
        for d in range(1, Y):
            fy_send(p, d, f).start()

    def relay(p):
        for d in range(1, Y):
            fy_recv(p, d).wait_recv()
            fc_send(p, d).start()

    def arrive(p):
        for f in range(NF):
            a_fold(p, f).wait_recv()
            forward(p, f)
        fc_send(p, 0).start()

    def norm(p):
        fc_recv(p).wait_recv()
        wide = x_all[span(p)].astype(F32)
        scale = lax.rsqrt(jnp.mean(wide * wide, axis=1, keepdims=True) + 1e-06)
        xn[span(p)] = (wide * scale * gain[...]).astype(BF16)

    TN = min(256, FL)
    NT = FL // TN

    def hidden(group, hooks):
        at = block(group)

        @pl.loop(0, NT)
        def _(n):
            nn = pl.ds(pl.multiple_of(n * TN, TN), TN)
            gate = jnp.dot(xn[at], wg[:, nn], preferred_element_type=F32)
            up = jnp.dot(xn[at], wu[:, nn], preferred_element_type=F32)
            act[at, nn] = (gate / (1.0 + jnp.exp(-gate)) * up).astype(BF16)
            for i in range(NT):
                todo = [hook for turn, hook in hooks if min(turn, NT - 1) == i]
                if todo:

                    @pl.when(n == i)
                    def _(todo=todo):
                        for hook in todo:
                            hook()

    def c2(g, d):
        at = block(groups[g])
        return remote(
            yp.at[at, cols(tp_of(yo(d), oc))], rc2.at[d, at], C2, c2_r.at[g, d], tp=tp_of(y, oc)
        )

    def down_block(g, tt):
        at = block(groups[g])
        yp[at, cols(tt)] = jnp.dot(act[at], wd[:, cols(tt)], preferred_element_type=F32).astype(
            BF16
        )

    def bwide(tt, f):
        return pl.ds(pl.multiple_of(tt * W + f * BW, BW), BW)

    def bfold(f):
        return pl.ds(f * BW, BW)

    def y2_send(p, d, f):
        return remote(
            sb2.at[d - 1, span(p), bfold(f)],
            ry2.at[seen(d), span(p), bfold(f)],
            Y2,
            y2_r.at[p, seen(d), f],
            tp=tp_of(yo(d), c),
        )

    def y2_recv(p, d, f):
        return remote(
            sb2.at[d - 1, span(p), bfold(f)],
            ry2.at[d - 1, span(p), bfold(f)],
            Y2,
            y2_r.at[p, d - 1, f],
            tp=tp_of(yo(d), c),
        )

    groups = [g for g in (first, second, third) if g]
    back = [g[:0:-1] + g[:1] if g is first else g[1:] + g[:1] for g in groups]

    def pair_sum(g, d):
        c2(g, d).wait_recv()
        for p in back[g]:
            at = span(p)
            sb2[d - 1, at] = (
                yp[at, cols(tp_of(yo(d), c))].astype(F32) + rc2[d, at].astype(F32)
            ).astype(BF16)
            if p:
                for f in range(NB):
                    y2_send(p, d, f).start()

    def y2_own(d):
        for f in range(NB):
            y2_send(0, d, f).start()

    def down(g, turn):
        for d in turn:
            down_block(g, tp_of(yo(d), oc))
            c2(g, d).start()
        for d in turn:
            down_block(g, tp_of(yo(d), c))

    def b_send(p, f):
        e = peer(p)
        return remote(
            rb.at[span(p), bfold(f)], ret.at[rows(me), bfold(f)], B, b_r.at[0], sp=e
        )

    def send_back(p):
        at = span(p)
        for f in range(NB):
            total = yp[at, bwide(t, f)].astype(F32) + rc2[0, at, bfold(f)].astype(F32)
            for d in range(1, Y):
                y2_recv(p, d, f).wait_recv()
                total = total + ry2[d - 1, at, bfold(f)].astype(F32)
            if p:
                rb[at, bfold(f)] = total.astype(BF16)
                b_send(p, f).start()
            else:
                ret[rows(me), bfold(f)] = total.astype(BF16)

    def later(f, *args):
        return lambda: f(*args)

    for f in range(NF):
        forward(0, f)
    fc_send(0, 0).start()
    for i, p in enumerate(arrivals):
        arrive(p)
        if i == 1:
            for q in third[1:]:
                for f in range(NF):
                    a_fold(q, f).start()
        if 1 <= i and p <= split:
            relay(p - 2)
    for p in range(min(split, Z) - 1, split):
        relay(p)
    for p in first:
        norm(p)
    loads[9].wait()
    loads[10].wait()
    steps = [later(arrive, p) for p in third[:1]] + [later(relay, p) for p in second]
    steps += [later(arrive, p) for p in third[1:2]]
    hidden(first, [(i, step) for i, step in enumerate(steps)])
    loads[11].wait()
    last = len(groups) - 1
    if second:
        for p in second:
            norm(p)
        steps = [later(arrive, p) for p in third[2:]] + [later(relay, p) for p in third[:-2]]
        hidden(second, [(i + 1, step) for i, step in enumerate(steps)])
        down(1, turns[:-1])
    else:
        for p in third[2:]:
            arrive(p)
        for p in third[:-2]:
            relay(p)
    down(0, turns[:-1])
    relay(third[-2])
    if second:
        for d in turns[:-1]:
            pair_sum(1, d)
        down(1, turns[-1:])
    for d in turns[:-1]:
        pair_sum(0, d)
    relay(third[-1])
    for p in third[:-1]:
        norm(p)
    down(0, turns[-1:])
    if second:
        c2(1, 0).wait_recv()
    norm(third[-1])
    steps = [later(send_back, p) for p in back[1]] if second else []
    hidden(third, [(NT - 2, step) for step in steps[:1]])
    down(last, turns[:-1])
    for step in steps[1:]:
        step()
    down_block(last, tp_of(y, oc))
    c2(last, 0).start()
    for d in turns[:-1]:
        pair_sum(last, d)
        y2_own(d)
    down_block(last, t)
    c2(0, 0).wait_recv()
    for p in back[0][:-1]:
        send_back(p)
    c2(last, 0).wait_recv()
    for p in back[-1] + [0]:
        send_back(p)

    others = pl.ds(0, (S - 1) * C)
    remote(rb.at[others], ret.at[others], B, b_r.at[0], sp=peer(1)).wait_recv()

    def gwide(tt, j):
        return pl.ds(pl.multiple_of(tt * W + j * GW, GW), GW)

    def gfold(j):
        return pl.ds(j * GW, GW)

    def gy_send(d, j):
        ref = out.at[:, gwide(t, j)]
        return remote(ref, ref, GY, gy_r.at[seen(d), j], tp=tp_of(yo(d), c))

    def gy_recv(d, j):
        ref = out.at[:, gwide(tp_of(yo(d), c), j)]
        return remote(ref, ref, GY, gy_r.at[d - 1, j], tp=tp_of(yo(d), c))

    def gc_send(d, j):
        ref = out.at[:, gwide(tp_of(yo(d), c), j)]
        return remote(ref, ref, GC, gc_r.at[0], tp=tp_of(y, oc))

    pick0 = picker(slot0).astype(BF16)
    pick1 = picker(slot1).astype(BF16)
    rw0 = column(rw[0:1, :])
    rw1 = column(rw[1:2, :])
    for j in range(NG):
        mix0 = jnp.dot(pick0, ret[:, gfold(j)], preferred_element_type=F32)
        mix1 = jnp.dot(pick1, ret[:, gfold(j)], preferred_element_type=F32)
        out[:, gwide(t, j)] = (
            mixed[:, gfold(j)].astype(F32) + (rw0 * mix0 + rw1 * mix1)
        ).astype(BF16)
        for d in range(1, Y):
            gy_send(d, j).start()
        gc_send(0, j).start()

    @pl.when(me < S - 1)
    def _():
        remote(halo, halo, HALO, halo_r.at[0], sp=me + 1).wait_send()

    def drain(ref, sem):
        remote(ref, ref, sem, sem, tp=tp_of(y, oc)).wait_send()

    drain(rc1, C1)
    drain(sb1.at[pl.ds(0, Y - 1)], Y1)
    drain(ret.at[others], A)
    drain(x_all.at[:, pl.ds(0, (Y - 1) * W)], FY)
    drain(x_all.at[:, pl.ds(0, Y * W)], FC)
    drain(x_all.at[:, pl.ds(0, Y * W)], C2)
    drain(x_all.at[:, pl.ds(0, (Y - 1) * W)], Y2)
    drain(ret.at[others], B)

    for j in range(NG):
        for d in range(1, Y):
            gy_recv(d, j).wait_recv()
            gc_send(d, j).start()
    ours = out.at[:, pl.ds(0, Y * W)]
    remote(ours, ours, GC, gc_r.at[0], tp=tp_of(y, oc)).wait_recv()
    drain(ours, GC)
    drain(out.at[:, pl.ds(0, (Y - 1) * W)], GY)


def per_device(
    S,
    T,
    queries,
    key_rows,
    value_rows,
    sink_logits,
    out_weight,
    residual,
    norm_gain,
    routes,
    route_weights,
    gate_weight,
    up_weight,
    down_weight,
):
    R, D = residual.shape
    HW = queries.shape[1]
    Y = T // CORES
    W = D // T
    C = 2 * R * TOP // S
    FL = gate_weight.shape[2]
    NH = 4 if W % 512 == 0 else 1
    NF = 2 if W % 256 == 0 else 1
    NG = 2 if W % 256 == 0 else 1
    NB = 2 if W % 256 == 0 else 1
    hbm = pl.BlockSpec(memory_space=pl.ANY)
    dma = pltpu.SemaphoreType.DMA
    v = pltpu.VMEM
    return pl.pallas_call(
        functools.partial(kernel, S, T),
        out_shape=v((R, D), BF16),
        in_specs=[hbm] * 12,
        out_specs=pl.BlockSpec(memory_space=v),
        scratch_shapes=[
            v((1, sink_logits.shape[0]), F32),
            v(queries.shape, BF16),
            v(key_rows.shape, BF16),
            v(value_rows.shape, BF16),
            v((R, W), BF16),
            v((1, D), F32),
            v((TOP, R), jnp.int32),
            v((TOP, R), F32),
            v(out_weight.shape, BF16),
            v(gate_weight.shape[1:], BF16),
            v(up_weight.shape[1:], BF16),
            v(down_weight.shape[1:], BF16),
            v((2,) + key_rows.shape, BF16),
            v((R, HW), BF16),
            v((R, D), BF16),
            v((Y, R, W), BF16),
            v((Y, NH, R, W // NH), BF16),
            v((Y, NH, R, W // NH), BF16),
            v((R, W), BF16),
            v((S * C, W), BF16),
            v((S * C, D), BF16),
            v((S * C, D), BF16),
            v((S * C, FL), BF16),
            v((S * C, D), BF16),
            v((Y, S * C, W), BF16),
            v((Y - 1, S * C, W), BF16),
            v((Y - 1, S * C, W), BF16),
            v((S * C, W), BF16),
            v((S * C, W), BF16),
            dma((12,)),
            pltpu.SemaphoreType.REGULAR((max(1, (S - 1).bit_length()),)),
            dma((11,)),
            dma((2,)),
            dma((Y,)),
            dma((Y - 1, NH)),
            dma((S, NF)),
            dma((S, Y - 1)),
            dma((S,)),
            dma((3, Y)),
            dma((S, Y - 1, NB)),
            dma((1,)),
            dma((Y - 1, NG)),
            dma((1,)),
        ],
        compiler_params=pltpu.CompilerParams(
            collective_id=0, has_side_effects=True, vmem_limit_bytes=60 * 1024 * 1024
        ),
        name="layer",
    )(
        sink_logits.reshape(1, -1),
        queries,
        key_rows,
        value_rows,
        residual,
        norm_gain.reshape(1, D),
        routes.T,
        route_weights.T,
        out_weight,
        gate_weight,
        up_weight,
        down_weight,
    )


def solution(mesh):
    placed = (
        P("sp", "tp"),
        P("sp", "tp"),
        P("sp", "tp"),
        P("tp"),
        P("tp", None),
        P("sp", None),
        P(),
        P("sp", None),
        P("sp", None),
        P("sp", None, "tp"),
        P("sp", None, "tp"),
        P("sp", "tp", None),
    )
    return jax.shard_map(
        functools.partial(per_device, mesh.shape["sp"], mesh.shape["tp"]),
        mesh=mesh,
        in_specs=placed,
        out_specs=P("sp", None),
        check_vma=False,
    )
```
